32 devices in a mesh: grp: 2 (over y), ep: 8 (over z, core), tp: 2 (over x).
Axes of the slice: x: 2, y: 2, z: 4, core: 2. Of those that a mesh axis runs over, the one named last changes fastest.
Arguments:
- tokens: bfloat16 [2048, 4096], P(('grp', 'ep'), 'tp'), parts along dimension 0, may hold values from -6 to 6
- routes: int32 [2048, 4], P(('grp', 'ep')), parts along dimension 0, may hold values from 0 to 7, all different within a row; in each aligned block of 128 rows (0 to 127, 128 to 255, ...) at most 128 rows name the same one
- route_weights: float32 [2048, 4], P(('grp', 'ep')), parts along dimension 0, may hold values from 0.1 to 1
- norm_gain: float32 [4096], replicated, may hold values from 0.1 to 1.9
- expert_gate: bfloat16 [8, 4096, 1024], P('ep', 'tp'), may hold values from -0.09375 to 0.09375
- expert_up: bfloat16 [8, 4096, 1024], P('ep', 'tp'), may hold values from -0.09375 to 0.09375
- expert_down: bfloat16 [8, 1024, 4096], P('ep', None, 'tp')
- shared_gate: bfloat16 [4096, 1024], P('tp'), may hold values from -0.09375 to 0.09375
- shared_up: bfloat16 [4096, 1024], P('tp'), may hold values from -0.09375 to 0.09375
- shared_down: bfloat16 [1024, 4096], P(None, 'tp')
- out_gain: float32 [4096], P('tp'), may hold values from 0.1 to 1.9
Outputs:
- layer_out: bfloat16 [2048, 4096], P(('grp', 'ep'), 'tp'), parts along dimension 0
The draws below stay inside these ranges and needn't reach their ends.
There are 2 independent parts, one for each index of `grp`. The reference program is written for one: setup_inputs(seed, part) draws one part's arguments, and reference() takes and returns one part's arrays. A program takes and returns all parts, laid end to end along the dimension named above; an argument that names none is the same for every part. Nothing has to cross between parts.
Inputs may be any that keep to these rules, and one draw needn't show every extreme that they name: `routes`: each row names 4 different experts; among the rows of one index of ep no expert is named more than 128 times, and in some such block some expert is named exactly 128 times.
All inputs are finite; a program needn't handle non-finite values.
Results may differ from the reference program's by a relative error of at most 0.023.
Values may be sent and summed in bfloat16 or wider, within the bound.
A program may use at most 64 MiB of HBM per device.

```python
import math
import jax
import jax.numpy as jnp
import numpy as np
from jax import lax

D = 4096
FF = 1024
FS = 1024
TOP_K = 4
TOK_EP = 128
EXPERTS = 8
CAP = 128
TOKENS = 1024
N_TP = 2


def rising_columns(key, width):
    base = jnp.exp(jnp.linspace(0.0, math.log(4.0), width, dtype=jnp.float32))
    jitter = jax.random.uniform(key, (width,), jnp.float32, 0.8, 1.2)
    return base * jitter


def draw_expert_down(key, part):
    noise = jax.random.normal(jax.random.fold_in(key, 11), (EXPERTS, FF, D), jnp.float32)
    rise = rising_columns(jax.random.fold_in(key, 12), D)
    return (noise * rise * FF ** (-0.5)).astype(jnp.bfloat16)


def draw_shared_down(key, part):
    noise = jax.random.normal(jax.random.fold_in(key, 21), (FS, D), jnp.float32)
    rise = rising_columns(jax.random.fold_in(key, 22), D)
    return (noise * rise * FS ** (-0.5)).astype(jnp.bfloat16)


def level_of(rng, extent, pieces, least, high):
    level = 1.0
    for position, shards_of in pieces:
        steps = jax.random.uniform(jax.random.fold_in(jax.random.fold_in(rng, 6), position), (shards_of,), jnp.float32, least / len(pieces), high / len(pieces))
        level = level * jnp.repeat(jnp.exp(steps), extent[position] // shards_of).reshape((-1,) + (1,) * (len(extent) - 1 - position))
    return level


def shared_out(own_key, own, number, rows, count, top, reach, lean):
    sequence = jax.random.permutation(own_key, count)
    crowded, usual = load_shares(count, rows * top, reach, lean, True), load_shares(count, rows * top, reach, lean, False)
    places = jnp.arange(count)

    def named(sizes, rotation):
        used = int((sizes > 0).sum())
        fixed = max(1, used // 4)
        shifted = fixed + (places - fixed + rotation * (used - fixed)) % max(1, count - fixed)
        return jnp.zeros((count,), jnp.int32).at[sequence[jnp.where(places < fixed, places, shifted)]].set(jnp.asarray(sizes, jnp.int32))

    sizes = jnp.where(number % 4 == 0, named(crowded, number // 4), named(usual, number - number // 4 - 1))
    mixed = jax.random.permutation(jax.random.fold_in(own, 3), count)
    giver, receiver = mixed[0:count // 2 * 2:2], mixed[1:count // 2 * 2:2]
    room = jnp.minimum(sizes[giver] - 1, reach - sizes[receiver]) // 2
    room = jnp.where((giver == sequence[0]) | (receiver == sequence[0]) | (sizes[receiver] == 0), 0, jnp.maximum(room, 0))
    shifted = jax.random.randint(jax.random.fold_in(own, 4), (count // 2,), 0, 1 << 20) % (room + 1)
    sizes = sizes.at[giver].add(-shifted).at[receiver].add(shifted)
    labels = jnp.searchsorted(jnp.cumsum(sizes), jnp.arange(rows * top), side="right").astype(jnp.int32)
    table = labels.reshape(top, rows).T
    table = table[jax.random.permutation(jax.random.fold_in(own, 1), rows)]
    rotation = jax.random.randint(jax.random.fold_in(own, 2), (rows, 1), 0, top)
    return jnp.take_along_axis(table, (jnp.arange(top)[None, :] + rotation) % top, axis=1)


def load_shares(number_of, total, reach, slope, full):
    portions = [(1 << 20) // math.isqrt(rank ** slope) + 1 for rank in range(1, number_of + 1)]
    largest = reach if full else min(reach, max(-(-total // number_of), total * portions[0] // sum(portions)))
    least = 1 if total - largest >= number_of - 1 else 0
    counts, surplus = [largest] + [least] * (number_of - 1), total - largest - least * (number_of - 1)
    while surplus > 0:
        candidates = [i for i in range(1, number_of) if counts[i] < largest] or [i for i in range(1, number_of) if counts[i] < reach]
        pool, remaining = sum([portions[i] for i in candidates]), surplus
        for i in candidates:
            more = min(reach - counts[i], max(1, remaining * portions[i] // pool), surplus)
            counts[i] = counts[i] + more
            surplus = surplus - more
    return np.array(counts)


def normal_values(rng, shape, deviation, reach, split=(), kind=jnp.bfloat16):
    gain = level_of(rng, shape, split, -0.22, 0.18) if split else 1.0
    values = jax.random.normal(rng, shape, jnp.float32) * deviation * gain
    return jnp.minimum(jnp.maximum(values, -reach), reach).astype(kind)


def setup_inputs(seed: int = 0, part: int = 0) -> dict:
    key_of = jax.random.split(jax.random.key(seed), 12)
    part_keys = jax.random.split(jax.random.fold_in(key_of[11], part), 12)
    tokens = normal_values(part_keys[0], (TOKENS, D), 1.0, 6.0, ((0, 8), (1, 2)))
    routes_keys = jax.random.split(jax.random.fold_in(part_keys[1], 1), TOKENS // TOK_EP)
    routes_turns = jax.random.permutation(jax.random.fold_in(part_keys[1], 3), TOKENS // TOK_EP)
    routes = jax.vmap(lambda own, number: shared_out(jax.random.fold_in(part_keys[1], 2), own, number, TOK_EP, EXPERTS, TOP_K, CAP, 2))(routes_keys, routes_turns).reshape((TOKENS, TOP_K))
    route_weights = jnp.clip(jnp.exp(math.log(1.0) - 2.3025851 * jax.random.uniform(part_keys[2], (TOKENS, TOP_K), jnp.float32) ** level_of(part_keys[2], (TOKENS, TOP_K), ((0, 8),), -0.2, 0.2)), 0.1, 1.0)
    norm_gain = jnp.clip(1.0 + 0.18 * jax.random.normal(key_of[3], (D,), jnp.float32), 0.1, 1.9)
    expert_gate = normal_values(key_of[4], (EXPERTS, D, FF), D ** -0.5, 0.09375, ((0, 8), (1, 2)))
    expert_up = normal_values(key_of[5], (EXPERTS, D, FF), D ** -0.5, 0.09375, ((0, 8), (1, 2)))
    expert_down = draw_expert_down(jax.random.fold_in(key_of[11], 71), part)
    shared_gate = normal_values(key_of[7], (D, FS), D ** -0.5, 0.09375, ((0, 2),))
    shared_up = normal_values(key_of[8], (D, FS), D ** -0.5, 0.09375, ((0, 2),))
    shared_down = draw_shared_down(jax.random.fold_in(key_of[11], 71), part)
    out_gain = jnp.clip(1.0 + 0.18 * jax.random.normal(key_of[10], (D,), jnp.float32), 0.1, 1.9)
    return dict(tokens=tokens, routes=routes, route_weights=route_weights, norm_gain=norm_gain, expert_gate=expert_gate, expert_up=expert_up, expert_down=expert_down, shared_gate=shared_gate, shared_up=shared_up, shared_down=shared_down, out_gain=out_gain)


epsilon = 1e-06

def blocked_product(source, matrix):
    rows = source.shape[0]
    source_blocks = source.reshape(rows, N_TP, -1).astype(jnp.float32)
    matrix_blocks = matrix.reshape(N_TP, -1, matrix.shape[1]).astype(jnp.float32)
    partial_value = jnp.einsum('rbf,bfh->brh', source_blocks, matrix_blocks)
    rounded = lax.optimization_barrier(partial_value.astype(jnp.bfloat16))
    return lax.optimization_barrier(jnp.sum(rounded.astype(jnp.float32), axis=0))

def expert_hidden(source, gate_matrix, up_matrix):
    gate_part = blocked_product(source, gate_matrix)
    up_part = blocked_product(source, up_matrix)
    return (jax.nn.silu(gate_part) * up_part).astype(jnp.bfloat16)

def reference(tokens, routes, route_weights, norm_gain, expert_gate, expert_up, expert_down, shared_gate, shared_up, shared_down, out_gain):
    full_float = tokens.astype(jnp.float32)
    normed = (full_float * lax.rsqrt(lax.optimization_barrier(jnp.mean(full_float * full_float, axis=-1, keepdims=True)) + epsilon) * norm_gain).astype(jnp.bfloat16)
    choose = (routes[:, :, None] == jnp.arange(EXPERTS, dtype=jnp.int32)[None, None, :]).astype(jnp.float32)
    weight_table = lax.optimization_barrier(jnp.sum(route_weights[:, :, None] * choose, axis=1))

    def add_expert(totals, expert):
        hidden = expert_hidden(normed, expert_gate[expert], expert_up[expert])
        expert_rows = jnp.dot(hidden, expert_down[expert], preferred_element_type=jnp.float32).astype(jnp.bfloat16)
        column = lax.dynamic_slice_in_dim(weight_table, expert, 1, 1)
        return (totals + column * expert_rows.astype(jnp.float32), None)
    routed, _ = lax.scan(add_expert, jnp.zeros((normed.shape[0], D), jnp.float32), jnp.arange(EXPERTS, dtype=jnp.int32))
    shared_hidden = expert_hidden(normed, shared_gate, shared_up)
    mixture = routed + jnp.dot(shared_hidden, shared_down, preferred_element_type=jnp.float32)
    scale = lax.rsqrt(lax.optimization_barrier(jnp.mean(mixture * mixture, axis=-1, keepdims=True)) + epsilon)
    return (mixture * scale * out_gain).astype(jnp.bfloat16)
```

```python
import functools

import jax
import jax.numpy as jnp
from jax import lax
from jax.experimental import pallas as pl
from jax.experimental.pallas import tpu as pltpu
from jax.sharding import PartitionSpec as P

epsilon = 1e-06
MESH = pl.DeviceIdType.MESH


def plan(chips):
    ring = [mask for mask in range(2, chips)]
    first = [(0, "own"), (1, 0)]
    last = [(1, 1), (0, "other"), None]
    steps = first + [(mask, 0) for mask in ring] + [(mask, 1) for mask in ring] + last
    relays = [[steps.index((distance, 0)), steps.index((max(distance, 2), 1))] for distance in range(1, chips)]
    relays[0][1] -= 1
    return steps, relays


def order(entry, core):
    mask, lane = (0, "own") if entry is None else entry
    return mask, core if lane == "own" else 1 - core if lane == "other" else lane


def pick(index, table):
    value = jnp.int32(table[0])
    for position in range(1, len(table)):
        if table[position] != table[0]:
            value = jnp.where(index == position, jnp.int32(table[position]), value)
    return value


def exclusive_or(a, b, size):
    total, unit = jnp.int32(0), 1
    while unit < size:
        total = total + unit * lax.rem(lax.div(a, unit) + lax.div(b, unit), 2)
        unit *= 2
    return total


def fused_kernel(
    chips,
    tokens_hbm,
    routes_hbm,
    weights_hbm,
    norm_gain_hbm,
    gate_hbm,
    up_hbm,
    down_hbm,
    shared_gate_hbm,
    shared_up_hbm,
    shared_down_hbm,
    out_gain_hbm,
    out_ref,
    routes_ref,
    weights_ref,
    norm_gain_ref,
    out_gain_ref,
    gate,
    up,
    down,
    held,
    source,
    part_out,
    part_in,
    part_own,
    hidden,
    product,
    waiting,
    pair_out,
    pair_in,
    far_out,
    far_in,
    mixture,
    square_out,
    square_in,
    info,
    load_sem,
    info_send,
    info_recv,
    square_send,
    square_recv,
    gather_send,
    gather_recv,
    pair_gather_recv,
    part_send,
    part_recv,
    hidden_send,
    hidden_recv,
    pair_send,
    pair_recv,
    far_send,
    far_recv,
):
    rows, width = mixture.shape
    experts = 2 * chips
    units = gate.shape[2]
    half = units // 2
    steps, relays = plan(chips)
    count = len(steps)
    masks = [order(entry, 0)[0] for entry in steps]
    lanes = [[order(entry, side)[1] for entry in steps] for side in range(2)]
    shared_at, other_at = steps.index(None), steps.index((0, "other"))

    ep = lax.axis_index("ep")
    tp = lax.axis_index("tp")
    chip, core = lax.div(ep, 2), lax.rem(ep, 2)
    other_core = 1 - core
    partner = {"ep": chip * 2 + other_core}
    across = {"tp": 1 - tp}

    away = pl.ds(pl.multiple_of((1 - tp) * half, half), half)
    near = pl.ds(pl.multiple_of(tp * half, half), half)
    features = pl.ds(pl.multiple_of(tp * width, width), width)
    loads = {
        name: pltpu.make_async_copy(source, target, load_sem.at[i])
        for i, (name, source, target) in enumerate(
            [
                ("tokens", tokens_hbm, held.at[ep]),
                ("norm_gain", norm_gain_hbm.at[:, features], norm_gain_ref),
                ("gate_away", gate_hbm.at[0, :, away], gate.at[0, :, away]),
                ("up_away", up_hbm.at[0, :, away], up.at[0, :, away]),
                ("gate_near", gate_hbm.at[0, :, near], gate.at[0, :, near]),
                ("up_near", up_hbm.at[0, :, near], up.at[0, :, near]),
                ("routes", routes_hbm, routes_ref),
                ("weights", weights_hbm, weights_ref),
                ("down", down_hbm.at[0], down.at[0]),
                ("shared_gate", shared_gate_hbm, gate.at[1]),
                ("shared_up", shared_up_hbm, up.at[1]),
                ("shared_down", shared_down_hbm, down.at[1]),
                ("out_gain", out_gain_hbm, out_gain_ref),
            ]
        )
    }
    for load in loads.values():
        load.start()

    barrier = pltpu.get_barrier_semaphore()
    for shift in range(1, experts):
        pl.semaphore_signal(
            barrier,
            inc=1,
            device_id={"ep": lax.rem(ep + shift, experts)},
            device_id_type=MESH,
        )
    pl.semaphore_signal(barrier, inc=1, device_id=across, device_id_type=MESH)

    def remote(source, target, send, recv, device):
        return pltpu.make_async_remote_copy(
            src_ref=source,
            dst_ref=target,
            send_sem=send,
            recv_sem=recv,
            device_id=device,
            device_id_type=MESH,
        )

    def square_copy(which):
        return remote(
            square_out.at[which],
            square_in.at[which],
            square_send.at[which],
            square_recv.at[which],
            across,
        )

    def info_copy(shift):
        return remote(
            info.at[ep],
            info.at[ep],
            info_send.at[shift],
            info_recv.at[ep],
            {"ep": lax.rem(ep + shift, experts)},
        )

    def info_arrival(block):
        return remote(info.at[block], info.at[block], info_send.at[0], info_recv.at[block], partner)

    def gather_copy(origin, way):
        slot = held.at[origin * 2 + core]
        device = ({"ep": (chip - 1) * 2 + core}, {"ep": (chip + 1) * 2 + core}, partner)[way]
        recv = (pair_gather_recv if way == 2 else gather_recv).at[origin]
        return remote(slot, slot, gather_send.at[origin, way], recv, device)

    def pair_gather_arrival(origin):
        slot = held.at[origin * 2 + other_core]
        return remote(slot, slot, gather_send.at[origin, 2], pair_gather_recv.at[origin], partner)

    def part_copy(k, which):
        return remote(
            part_out.at[k, which],
            part_in.at[k, which],
            part_send.at[k, which],
            part_recv.at[k, which],
            across,
        )

    def hidden_copy(k, side):
        return remote(
            hidden.at[k, side], hidden.at[k, side], hidden_send.at[k], hidden_recv.at[k], across
        )

    def pair_copy(origin):
        return remote(
            pair_out.at[origin],
            pair_in.at[origin],
            pair_send.at[origin],
            pair_recv.at[origin],
            partner,
        )

    beside, opposite, beyond = (exclusive_or(chip, mask, chips) for mask in (1, 2, 3))

    def far_copy(mask, origin):
        slot = jnp.where(mask == 2, beyond, chip)
        return remote(
            far_out.at[origin],
            far_in.at[slot],
            far_send.at[origin],
            far_recv.at[slot],
            {"ep": jnp.where(mask == 3, beyond, beside) * 2 + core},
        )

    def far_arrival(slot):
        return remote(
            far_out.at[slot],
            far_in.at[slot],
            far_send.at[slot],
            far_recv.at[slot],
            {"ep": beside * 2 + core},
        )

    def pack(column):
        return jnp.transpose(jnp.broadcast_to(column, (rows, 128)))[:8]

    def unpack(row):
        return jnp.transpose(jnp.broadcast_to(row[:1], (128, rows)))[:, :1]

    loads["tokens"].wait()
    token_float = held[ep].astype(jnp.float32)
    own_square = jnp.sum(token_float * token_float, axis=-1, keepdims=True)
    square_out[0] = pack(own_square)
    pl.semaphore_wait(barrier, experts)

    def send_outward():
        @pl.when(chip > 0)
        def _():
            gather_copy(chip, 0).start()

        @pl.when(chip < chips - 1)
        def _():
            gather_copy(chip, 1).start()

    pl.when(core == 0)(send_outward)
    gather_copy(chip, 2).start()
    square_copy(0).start()
    loads["norm_gain"].wait()

    def share_info():
        loads["routes"].wait()
        loads["weights"].wait()
        expert_ids = lax.broadcasted_iota(jnp.int32, (experts, rows), 0)
        table = jnp.zeros((experts, rows), jnp.float32)
        for choice in range(routes_ref.shape[0]):
            match = expert_ids == routes_ref[choice : choice + 1, :]
            table = table + jnp.where(match, weights_ref[choice : choice + 1, :], 0.0)
        info[ep, :experts] = table
        square_copy(0).wait_recv()
        square = square_out[0] + square_in[0]
        info[ep, experts:] = lax.rsqrt(square / (2 * width) + epsilon)
        for shift in range(1, experts):
            info_copy(shift).start()

    def locate(k):
        origin = exclusive_or(chip, pick(k, masks), chips)
        lane = jnp.where(core == 0, pick(k, lanes[0]), pick(k, lanes[1]))
        return origin, lane

    def block_of(k):
        origin, lane = locate(k)
        return jnp.where(k == shared_at, ep, origin * 2 + lane)

    def first_stage(k):
        origin, lane = locate(k)
        is_shared = k == shared_at

        @pl.when(is_shared)
        def _():
            loads["shared_gate"].wait()
            loads["shared_up"].wait()

        for index, positions in enumerate(relays):
            distance = index + 1
            position = jnp.where(core == 0, positions[0], positions[1])

            @pl.when((k == position) & (chip >= distance))
            def _(distance=distance):
                gather_copy(chip - distance, 0).wait_recv()
                gather_copy(chip - distance, 2).start()

                @pl.when(chip < chips - 1)
                def _():
                    gather_copy(chip - distance, 1).start()

            @pl.when((k == position) & (chip + distance < chips))
            def _(distance=distance):
                gather_copy(chip + distance, 1).wait_recv()
                gather_copy(chip + distance, 2).start()

                @pl.when(chip > 0)
                def _():
                    gather_copy(chip + distance, 0).start()

        @pl.when((lane != core) & (k != shared_at))
        def _():
            pair_gather_arrival(origin).wait_recv()

        block = block_of(k)
        kind = jnp.where(is_shared, 1, 0)
        source[...] = (held[block].astype(jnp.float32) * norm_gain_ref[...]).astype(jnp.bfloat16)
        for which, matrix, name in ((0, gate, "gate_away"), (1, up, "up_away")):
            pl.when(k == 0)(loads[name].wait)
            part_out[k, which] = jnp.dot(
                source[...], matrix[kind, :, away], preferred_element_type=jnp.float32
            ).astype(jnp.bfloat16)
            part_copy(k, which).start()
        for which, matrix, name in ((0, gate, "gate_near"), (1, up, "up_near")):
            pl.when(k == 0)(loads[name].wait)
            part_own[k, which] = jnp.dot(
                source[...], matrix[kind, :, near], preferred_element_type=jnp.float32
            ).astype(jnp.bfloat16)

    def second_stage(k):
        block = block_of(k)

        @pl.when(block != ep)
        def _():
            info_arrival(block).wait_recv()

        scale = unpack(info[block, experts : experts + 1])
        part_copy(k, 0).wait_recv()
        part_copy(k, 1).wait_recv()
        gate_sum = part_own[k, 0].astype(jnp.float32) + part_in[k, 0].astype(jnp.float32)
        up_sum = part_own[k, 1].astype(jnp.float32) + part_in[k, 1].astype(jnp.float32)
        gate_sum, up_sum = gate_sum * scale, up_sum * scale
        hidden[k, tp] = (jax.nn.silu(gate_sum) * up_sum).astype(jnp.bfloat16)
        hidden_copy(k, tp).start()

    def third_stage(k):
        origin, lane = locate(k)
        is_shared = k == shared_at

        pl.when(k == 0)(loads["down"].wait)
        pl.when(is_shared)(loads["shared_down"].wait)
        kind = jnp.where(is_shared, 1, 0)
        tile = width // 4

        def own_step(i, carry):
            columns = pl.ds(pl.multiple_of(i * tile, tile), tile)
            product[:, columns] = jnp.dot(
                hidden[k, tp], down[kind, near, columns], preferred_element_type=jnp.float32
            )
            return carry

        def other_step(i, carry):
            columns = pl.ds(pl.multiple_of(i * tile, tile), tile)
            product[:, columns] += jnp.dot(
                hidden[k, 1 - tp], down[kind, away, columns], preferred_element_type=jnp.float32
            )
            return carry

        lax.fori_loop(0, 4, own_step, 0)
        scale = unpack(info[block_of(k), pl.ds(ep, 1)])
        hidden_copy(k, 1 - tp).wait_recv()
        lax.fori_loop(0, 4, other_step, 0)

        def weighted():
            return product[...].astype(jnp.bfloat16).astype(jnp.float32) * scale

        @pl.when(is_shared)
        def _():
            mixture[...] += product[...]

        @pl.when((k != shared_at) & (lane != core))
        def _():
            pair_out[origin] = weighted().astype(jnp.bfloat16)
            pair_copy(origin).start()

        @pl.when(k == 0)
        def _():
            mixture[...] = weighted()

        @pl.when((k != 0) & (k != shared_at) & (lane == core))
        def _():
            waiting[...] = weighted()

    def fourth_stage(k):
        origin, lane = locate(k)

        @pl.when(k == other_at)
        def _():
            pair_copy(chip).wait_recv()
            mixture[...] += pair_in[chip].astype(jnp.float32)

        @pl.when((k != 0) & (k != shared_at) & (lane == core))
        def _():
            pair_copy(origin).wait_recv()
            mask = pick(k, masks)

            @pl.when(mask == 3)
            def _():
                far_arrival(opposite).wait_recv()
                waiting[...] += far_in[opposite].astype(jnp.float32)

            far_out[origin] = (waiting[...] + pair_in[origin].astype(jnp.float32)).astype(
                jnp.bfloat16
            )
            far_copy(mask, origin).start()

    def body(i, carry):
        @pl.when(i < count)
        def _():
            first_stage(i)

        pl.when(i == 0)(share_info)

        @pl.when(i >= 3)
        def _():
            fourth_stage(i - 3)

        @pl.when((i >= 1) & (i < count + 1))
        def _():
            second_stage(i - 1)

        @pl.when((i == 1) & (core == 1))
        def _():
            send_outward()

        @pl.when((i >= 2) & (i < count + 2))
        def _():
            third_stage(i - 2)

        return carry

    lax.fori_loop(0, count + 3, body, 0)

    far_arrival(beside).wait_recv()
    far_arrival(beyond).wait_recv()
    mixture[...] += far_in[beside].astype(jnp.float32) + far_in[beyond].astype(jnp.float32)

    mixed = mixture[...]
    own_total = jnp.sum(mixed * mixed, axis=-1, keepdims=True)
    square_out[1] = pack(own_total)
    square_copy(1).start()
    loads["out_gain"].wait()
    square_copy(1).wait_recv()
    total = own_total + unpack(square_in[1])
    out_ref[...] = (
        mixture[...] * lax.rsqrt(total / (2 * width) + epsilon) * out_gain_ref[...]
    ).astype(jnp.bfloat16)

    square_copy(0).wait_send()
    square_copy(1).wait_send()
    for shift in range(1, experts):
        info_copy(shift).wait_send()
    for origin in range(chips):
        gather_copy(origin, 2).wait_send()
        pair_copy(origin).wait_send()

        @pl.when((chip >= origin) & (chip < chips - 1))
        def _(origin=origin):
            gather_copy(origin, 1).wait_send()

        @pl.when((chip <= origin) & (chip > 0))
        def _(origin=origin):
            gather_copy(origin, 0).wait_send()

        @pl.when(chip != origin)
        def _(origin=origin):
            far_arrival(origin).wait_send()

    def drain(k, carry):
        part_copy(k, 0).wait_send()
        part_copy(k, 1).wait_send()
        hidden_copy(k, tp).wait_send()
        return carry

    lax.fori_loop(0, count, drain, 0)


def fused(
    chips,
    tokens,
    routes,
    route_weights,
    norm_gain,
    expert_gate,
    expert_up,
    expert_down,
    shared_gate,
    shared_up,
    shared_down,
    out_gain,
):
    rows, width = tokens.shape
    units = shared_gate.shape[1]
    half = units // 2
    count = 2 * chips + 1
    choices = routes.shape[1]
    vmem = pl.BlockSpec(memory_space=pltpu.VMEM)
    hbm = pl.BlockSpec(memory_space=pl.ANY)
    bf16, f32 = jnp.bfloat16, jnp.float32
    dma = pltpu.SemaphoreType.DMA
    return pl.pallas_call(
        functools.partial(fused_kernel, chips),
        out_shape=pltpu.VMEM((rows, width), bf16),
        in_specs=[hbm] * 11,
        out_specs=vmem,
        scratch_shapes=[
            pltpu.VMEM((choices, rows), jnp.int32),
            pltpu.VMEM((choices, rows), f32),
            pltpu.VMEM((1, width), f32),
            pltpu.VMEM((1, width), f32),
            pltpu.VMEM((2, width, units), bf16),
            pltpu.VMEM((2, width, units), bf16),
            pltpu.VMEM((2, units, width), bf16),
            pltpu.VMEM((2 * chips, rows, width), bf16),
            pltpu.VMEM((rows, width), bf16),
            pltpu.VMEM((count, 2, rows, half), bf16),
            pltpu.VMEM((count, 2, rows, half), bf16),
            pltpu.VMEM((count, 2, rows, half), bf16),
            pltpu.VMEM((count, 2, rows, half), bf16),
            pltpu.VMEM((rows, width), f32),
            pltpu.VMEM((rows, width), f32),
            pltpu.VMEM((chips, rows, width), bf16),
            pltpu.VMEM((chips, rows, width), bf16),
            pltpu.VMEM((chips, rows, width), bf16),
            pltpu.VMEM((chips, rows, width), bf16),
            pltpu.VMEM((rows, width), f32),
            pltpu.VMEM((2, 8, rows), f32),
            pltpu.VMEM((2, 8, rows), f32),
            pltpu.VMEM((2 * chips, 2 * chips + 8, rows), f32),
            dma((13,)),
            dma((2 * chips,)),
            dma((2 * chips,)),
            dma((2,)),
            dma((2,)),
            dma((chips, 3)),
            dma((chips,)),
            dma((chips,)),
            dma((count, 2)),
            dma((count, 2)),
            dma((count,)),
            dma((count,)),
            dma((chips,)),
            dma((chips,)),
            dma((chips,)),
            dma((chips,)),
        ],
        compiler_params=pltpu.CompilerParams(
            collective_id=0, has_side_effects=True, vmem_limit_bytes=60 * 1024 * 1024
        ),
    )(
        tokens,
        routes.T,
        route_weights.T,
        norm_gain.reshape(1, -1),
        expert_gate,
        expert_up,
        expert_down,
        shared_gate,
        shared_up,
        shared_down,
        out_gain.reshape(1, -1),
    )


def local_product(source, matrix):
    return jnp.dot(source, matrix, preferred_element_type=jnp.float32)


def per_device(
    tokens,
    routes,
    route_weights,
    norm_gain,
    expert_gate,
    expert_up,
    expert_down,
    shared_gate,
    shared_up,
    shared_down,
    out_gain,
):
    block_width = tokens.shape[1]
    full_width = block_width * lax.axis_size("tp")
    width_index = lax.axis_index("tp")
    full_rows = lax.all_gather(tokens, "tp", axis=1, tiled=True)
    full_float = full_rows.astype(jnp.float32)
    normed_full = (
        full_float
        * lax.rsqrt(jnp.mean(full_float * full_float, axis=-1, keepdims=True) + epsilon)
        * norm_gain
    ).astype(jnp.bfloat16)
    normed_block = lax.dynamic_slice_in_dim(normed_full, width_index * block_width, block_width, 1)
    gate_matrix = expert_gate[0]
    up_matrix = expert_up[0]
    down_matrix = expert_down[0]
    experts = lax.axis_size("ep")
    choose = (routes[:, :, None] == jnp.arange(experts, dtype=jnp.int32)[None, None, :]).astype(
        jnp.float32
    )
    weight_table = jnp.sum(route_weights[:, :, None] * choose, axis=1)
    expert_input = lax.all_gather(normed_block, "ep", axis=0, tiled=True)
    table_all = lax.all_gather(weight_table, "ep", axis=0, tiled=True)
    summed = (
        lax.psum(local_product(expert_input, gate_matrix).astype(jnp.bfloat16), "tp").astype(
            jnp.float32
        ),
        lax.psum(local_product(expert_input, up_matrix).astype(jnp.bfloat16), "tp").astype(
            jnp.float32
        ),
        lax.psum(local_product(normed_block, shared_gate).astype(jnp.bfloat16), "tp").astype(
            jnp.float32
        ),
        lax.psum(local_product(normed_block, shared_up).astype(jnp.bfloat16), "tp").astype(
            jnp.float32
        ),
    )
    routed_hidden = (jax.nn.silu(summed[0]) * summed[1]).astype(jnp.bfloat16)
    shared_hidden = (jax.nn.silu(summed[2]) * summed[3]).astype(jnp.bfloat16)
    expert_rows = local_product(routed_hidden, down_matrix).astype(jnp.bfloat16)
    shared_out = local_product(shared_hidden, shared_down)
    own_expert = lax.axis_index("ep")
    column = lax.dynamic_slice_in_dim(table_all, own_expert, 1, 1)
    routed = lax.psum_scatter(
        (column * expert_rows.astype(jnp.float32)).astype(jnp.bfloat16),
        "ep",
        scatter_dimension=0,
        tiled=True,
    ).astype(jnp.float32)
    mixture = routed + shared_out
    square_sum = lax.psum(jnp.sum(mixture * mixture, axis=-1, keepdims=True), "tp")
    scale = lax.rsqrt(square_sum / full_width + epsilon)
    return (mixture * scale * out_gain).astype(jnp.bfloat16)


def solution(mesh):
    chips = mesh.shape["ep"] // 2
    if mesh.shape["tp"] == 2 and mesh.shape["ep"] == 8:
        body = functools.partial(fused, chips)
    else:
        body = per_device
    return jax.shard_map(
        body,
        mesh=mesh,
        in_specs=(
            P(("grp", "ep"), "tp"),
            P(("grp", "ep"), None),
            P(("grp", "ep"), None),
            P(),
            P("ep", "tp", None),
            P("ep", "tp", None),
            P("ep", None, "tp"),
            P("tp", None),
            P("tp", None),
            P(None, "tp"),
            P("tp"),
        ),
        out_specs=P(("grp", "ep"), "tp"),
        check_vma=False,
    )
```

```python
import functools

import jax
import jax.numpy as jnp
from jax import lax
from jax.experimental import pallas as pl
from jax.experimental.pallas import tpu as pltpu
from jax.sharding import PartitionSpec as P

epsilon = 1e-06
MESH = pl.DeviceIdType.MESH


NEAR, MIDDLE, FAR = range(3)
STEPS = (
    "own",
    (NEAR, 0),
    (MIDDLE, 0),
    (FAR, 0),
    (FAR, 1),
    (MIDDLE, 1),
    (NEAR, 1),
    "other",
    "shared",
)


def pick(index, table):
    value = jnp.int32(table[0])
    for position in range(1, len(table)):
        if table[position] != table[0]:
            value = jnp.where(index == position, jnp.int32(table[position]), value)
    return value


def exclusive_or(a, b, size):
    total, unit = jnp.int32(0), 1
    while unit < size:
        total = total + unit * lax.rem(lax.div(a, unit) + lax.div(b, unit), 2)
        unit *= 2
    return total


def fused_kernel(
    chips,
    tokens_hbm,
    routes_hbm,
    weights_hbm,
    norm_gain_hbm,
    gate_hbm,
    up_hbm,
    down_hbm,
    shared_gate_hbm,
    shared_up_hbm,
    shared_down_hbm,
    out_gain_hbm,
    out_ref,
    routes_ref,
    weights_ref,
    norm_gain_ref,
    out_gain_ref,
    gate,
    up,
    down,
    held,
    source,
    part_out,
    part_in,
    part_own,
    hidden,
    product,
    waiting,
    pair_out,
    pair_in,
    far_out,
    far_in,
    mixture,
    square_out,
    square_in,
    info_out,
    info,
    load_sem,
    info_send,
    info_recv,
    square_send,
    square_recv,
    gather_send,
    gather_recv,
    pair_gather_recv,
    part_send,
    part_recv,
    hidden_send,
    hidden_recv,
    pair_send,
    pair_recv,
    far_send,
    far_recv,
):
    rows, width = mixture.shape
    experts = 2 * chips
    units = gate.shape[2]
    half = units // 2
    count = len(STEPS)
    slots = [step[0] if isinstance(step, tuple) else NEAR for step in STEPS]
    lanes = [
        [side if step == "own" else 1 - side if step == "other" else step[1] if isinstance(step, tuple) else side for step in STEPS]
        for side in range(2)
    ]
    shared_at, other_at = STEPS.index("shared"), STEPS.index("other")

    ep = lax.axis_index("ep")
    tp = lax.axis_index("tp")
    chip, core = lax.div(ep, 2), lax.rem(ep, 2)
    other_core = 1 - core
    partner = {"ep": chip * 2 + other_core}
    across = {"tp": 1 - tp}

    away = pl.ds(pl.multiple_of((1 - tp) * half, half), half)
    near = pl.ds(pl.multiple_of(tp * half, half), half)
    features = pl.ds(pl.multiple_of(tp * width, width), width)
    loads = {
        name: pltpu.make_async_copy(source, target, load_sem.at[i])
        for i, (name, source, target) in enumerate(
            [
                ("tokens", tokens_hbm, held.at[ep]),
                ("norm_gain", norm_gain_hbm.at[:, features], norm_gain_ref),
                ("gate_away", gate_hbm.at[0, :, away], gate.at[0, :, away]),
                ("up_away", up_hbm.at[0, :, away], up.at[0, :, away]),
                ("gate_near", gate_hbm.at[0, :, near], gate.at[0, :, near]),
                ("up_near", up_hbm.at[0, :, near], up.at[0, :, near]),
                ("routes", routes_hbm, routes_ref),
                ("weights", weights_hbm, weights_ref),
                ("down", down_hbm.at[0], down.at[0]),
                ("shared_gate", shared_gate_hbm, gate.at[1]),
                ("shared_up", shared_up_hbm, up.at[1]),
                ("shared_down", shared_down_hbm, down.at[1]),
                ("out_gain", out_gain_hbm, out_gain_ref),
            ]
        )
    }
    for load in loads.values():
        load.start()

    barrier = pltpu.get_barrier_semaphore()
    for shift in range(1, experts):
        pl.semaphore_signal(
            barrier,
            inc=1,
            device_id={"ep": lax.rem(ep + shift, experts)},
            device_id_type=MESH,
        )
    pl.semaphore_signal(barrier, inc=1, device_id=across, device_id_type=MESH)

    def remote(source, target, send, recv, device):
        return pltpu.make_async_remote_copy(
            src_ref=source,
            dst_ref=target,
            send_sem=send,
            recv_sem=recv,
            device_id=device,
            device_id_type=MESH,
        )

    def square_copy(which):
        return remote(
            square_out.at[which],
            square_in.at[which],
            square_send.at[which],
            square_recv.at[which],
            across,
        )

    def info_copy(shift):
        return remote(
            info_out.at[shift],
            info.at[ep],
            info_send.at[shift],
            info_recv.at[ep],
            {"ep": lax.rem(ep + shift, experts)},
        )

    def info_arrival(block):
        return remote(info.at[block], info.at[block], info_send.at[0], info_recv.at[block], partner)

    def gather_copy(origin, way):
        slot = held.at[origin * 2 + core]
        device = ({"ep": (chip - 1) * 2 + core}, {"ep": (chip + 1) * 2 + core}, partner)[way]
        recv = (pair_gather_recv if way == 2 else gather_recv).at[origin]
        return remote(slot, slot, gather_send.at[origin, way], recv, device)

    def pair_gather_arrival(origin):
        slot = held.at[origin * 2 + other_core]
        return remote(slot, slot, gather_send.at[origin, 2], pair_gather_recv.at[origin], partner)

    def part_copy(k, which):
        return remote(
            part_out.at[k, which],
            part_in.at[k, which],
            part_send.at[k, which],
            part_recv.at[k, which],
            across,
        )

    def hidden_copy(k, side):
        return remote(
            hidden.at[k, side], hidden.at[k, side], hidden_send.at[k], hidden_recv.at[k], across
        )

    def pair_copy(origin):
        return remote(
            pair_out.at[origin],
            pair_in.at[origin],
            pair_send.at[origin],
            pair_recv.at[origin],
            partner,
        )

    beside, opposite, beyond = (exclusive_or(chip, mask, chips) for mask in (1, 2, 3))
    outer = (chip == 0) | (chip == chips - 1)
    inner = jnp.logical_not(outer)

    def origin_of(slot):
        middle, far = jnp.where(outer, opposite, beyond), jnp.where(outer, beyond, opposite)
        return jnp.where(slot == NEAR, beside, jnp.where(slot == MIDDLE, middle, far))

    def far_copy(slot):
        direct = outer | (slot == NEAR)
        place = jnp.where(direct, slot, FAR + 1)
        target = jnp.where(direct, beside, origin_of(slot))
        return remote(
            far_out.at[slot],
            far_in.at[place],
            far_send.at[slot],
            far_recv.at[place],
            {"ep": target * 2 + core},
        )

    def far_arrival(place):
        return remote(
            far_out.at[0],
            far_in.at[place],
            far_send.at[0],
            far_recv.at[place],
            {"ep": beside * 2 + core},
        )

    def pack(column):
        return jnp.transpose(jnp.broadcast_to(column, (rows, 128)))[:8]

    def unpack(row):
        return jnp.transpose(jnp.broadcast_to(row[:1], (128, rows)))[:, :1]

    loads["tokens"].wait()
    token_float = held[ep].astype(jnp.float32)
    own_square = jnp.sum(token_float * token_float, axis=-1, keepdims=True)
    square_out[0] = pack(own_square)
    pl.semaphore_wait(barrier, experts)

    def send_outward():
        @pl.when(chip > 0)
        def _():
            gather_copy(chip, 0).start()

        @pl.when(chip < chips - 1)
        def _():
            gather_copy(chip, 1).start()

    pl.when(core == 0)(send_outward)
    gather_copy(chip, 2).start()
    square_copy(0).start()
    loads["norm_gain"].wait()

    def share_info():
        loads["routes"].wait()
        loads["weights"].wait()
        square_copy(0).wait_recv()
        square = square_out[0] + square_in[0]
        scale = lax.rsqrt(square / (2 * width) + epsilon)
        first_row = lax.broadcasted_iota(jnp.int32, scale.shape, 0) == 0
        for shift in range(experts):
            named = routes_ref[...] == lax.rem(ep + shift, experts)
            weight = jnp.sum(jnp.where(named, weights_ref[...], 0.0), axis=0, keepdims=True)
            message = jnp.where(first_row, weight, scale)
            if shift == 0:
                info[ep] = message
            else:
                info_out[shift] = message
                info_copy(shift).start()

    def take(origin):
        gather_copy(origin, 0).wait_recv()
        gather_copy(origin, 2).start()

    def toward_outer(origin):
        @pl.when(chip == 1)
        def _():
            gather_copy(origin, 0).start()

        @pl.when(chip == chips - 2)
        def _():
            gather_copy(origin, 1).start()

    def toward_inner(origin):
        @pl.when(chip < chips // 2)
        def _():
            gather_copy(origin, 1).start()

        @pl.when(chip >= chips // 2)
        def _():
            gather_copy(origin, 0).start()

    def relay(distance):
        @pl.when(chip >= distance)
        def _():
            take(chip - distance)

            @pl.when(chip < chips - 1)
            def _():
                gather_copy(chip - distance, 1).start()

        @pl.when(chip + distance < chips)
        def _():
            take(chip + distance)

            @pl.when(chip > 0)
            def _():
                gather_copy(chip + distance, 0).start()

    def second_lane_between(i):
        @pl.when((i == 1) & outer)
        def _():
            toward_inner(chip)

        @pl.when((i == 2) & inner)
        def _():
            take(beside)
            toward_inner(beside)
            toward_inner(chip)

        @pl.when((i == 4) & inner)
        def _():
            take(beyond)
            toward_outer(beyond)
            toward_outer(chip)

    def second_lane_after(i):
        @pl.when((i == 3) & inner)
        def _():
            take(opposite)
            toward_outer(opposite)

        @pl.when((i >= 3) & (i < 6) & outer)
        def _():
            take(origin_of(pick(i + 1, slots)))

    def locate(k):
        away_from = origin_of(pick(k, slots))
        origin = jnp.where((k == 0) | (k >= other_at), chip, away_from)
        lane = jnp.where(core == 0, pick(k, lanes[0]), pick(k, lanes[1]))
        return origin, lane

    def block_of(k):
        origin, lane = locate(k)
        return jnp.where(k == shared_at, ep, origin * 2 + lane)

    def first_stage(k):
        origin, lane = locate(k)
        is_shared = k == shared_at

        @pl.when(is_shared)
        def _():
            loads["shared_gate"].wait()
            loads["shared_up"].wait()

        pl.when((k == 2) & (core == 0) & outer)(functools.partial(relay, 2))
        pl.when((k == 3) & (core == 0))(functools.partial(relay, 3))

        @pl.when((lane != core) & (k != shared_at))
        def _():
            pair_gather_arrival(origin).wait_recv()

        block = block_of(k)
        kind = jnp.where(is_shared, 1, 0)
        source[...] = (held[block].astype(jnp.float32) * norm_gain_ref[...]).astype(jnp.bfloat16)
        for which, matrix, name in ((0, gate, "gate_away"), (1, up, "up_away")):
            pl.when(k == 0)(loads[name].wait)
            part_out[k, which] = jnp.dot(
                source[...], matrix[kind, :, away], preferred_element_type=jnp.float32
            ).astype(jnp.bfloat16)
            part_copy(k, which).start()
        for which, matrix, name in ((0, gate, "gate_near"), (1, up, "up_near")):
            pl.when(k == 0)(loads[name].wait)
            part_own[k, which] = jnp.dot(
                source[...], matrix[kind, :, near], preferred_element_type=jnp.float32
            ).astype(jnp.bfloat16)

    def second_stage(k):
        block = block_of(k)

        @pl.when(block != ep)
        def _():
            info_arrival(block).wait_recv()

        scale = unpack(info[block, 1:2])
        part_copy(k, 0).wait_recv()
        part_copy(k, 1).wait_recv()
        gate_sum = part_own[k, 0].astype(jnp.float32) + part_in[k, 0].astype(jnp.float32)
        up_sum = part_own[k, 1].astype(jnp.float32) + part_in[k, 1].astype(jnp.float32)
        gate_sum, up_sum = gate_sum * scale, up_sum * scale
        hidden[k, tp] = (jax.nn.silu(gate_sum) * up_sum).astype(jnp.bfloat16)
        hidden_copy(k, tp).start()

    def down_product(k, side, columns):
        rows_of = pl.ds(pl.multiple_of(side * half, half), half)
        kind = jnp.where(k == shared_at, 1, 0)
        return jnp.dot(
            hidden[k, side], down[kind, rows_of, columns], preferred_element_type=jnp.float32
        )

    tile = width // 4

    def tiles(step):
        def tile_step(i, carry):
            step(pl.ds(pl.multiple_of(i * tile, tile), tile))
            return carry

        lax.fori_loop(0, 4, tile_step, 0)

    def third_stage(k):
        origin, lane = locate(k)
        pl.when(k == 0)(loads["down"].wait)

        def own_step(columns):
            product[:, columns] = down_product(k, tp, columns)

        def other_step(columns):
            product[:, columns] += down_product(k, 1 - tp, columns)

        tiles(own_step)
        scale = unpack(info[block_of(k), :1])
        hidden_copy(k, 1 - tp).wait_recv()
        tiles(other_step)

        def weighted():
            return product[...].astype(jnp.bfloat16).astype(jnp.float32) * scale

        @pl.when(lane != core)
        def _():
            pair_out[origin] = weighted().astype(jnp.bfloat16)
            pair_copy(origin).start()

        @pl.when(k == 0)
        def _():
            mixture[...] = weighted()

        @pl.when((k != 0) & (lane == core))
        def _():
            waiting[pick(k, slots)] = weighted()

    def fourth_stage(k):
        origin, lane = locate(k)

        @pl.when((k != 0) & (lane == core))
        def _():
            slot = pick(k, slots)
            pair_copy(origin).wait_recv()
            waiting[slot] += pair_in[origin].astype(jnp.float32)

            @pl.when(outer | (slot == NEAR))
            def _():
                far_out[slot] = waiting[slot].astype(jnp.bfloat16)

            @pl.when((outer | (slot == NEAR)) & (k != 1))
            def _():
                far_copy(slot).start()

    def fifth_stage(k):
        slot = pick(k, slots)
        far_arrival(slot).wait_recv()
        far_out[slot] = (waiting[slot] + far_in[slot].astype(jnp.float32)).astype(jnp.bfloat16)
        far_copy(slot).start()

    def body(i, carry):
        @pl.when(i == 1)
        def _():
            pl.when(core == 0)(functools.partial(relay, 1))
            second_stage(0)

        @pl.when(i < count)
        def _():
            first_stage(i)

        pl.when(core == 1)(functools.partial(second_lane_between, i))
        pl.when(i == 0)(share_info)

        @pl.when(i >= 3)
        def _():
            fourth_stage(i - 3)

        @pl.when((i == 5) & (core == 0))
        def _():
            far_copy(NEAR).start()

        @pl.when(inner & jnp.where(core == 0, (i == 7) | (i == 8), (i == 8) | (i == 9)))
        def _():
            fifth_stage(i - 5 + core)

        pl.when((i == 2) & (core == 0) & inner)(functools.partial(relay, 2))

        @pl.when((i >= 2) & (i < count + 1))
        def _():
            second_stage(i - 1)

        pl.when(core == 1)(functools.partial(second_lane_after, i))

        @pl.when(i >= 2)
        def _():
            third_stage(i - 2)

        return carry

    lax.fori_loop(0, count + 1, body, 0)

    def shared_own(columns):
        mixture[:, columns] += down_product(shared_at, tp, columns)

    loads["shared_down"].wait()
    tiles(shared_own)
    pair_copy(chip).wait_recv()
    mixture[...] += pair_in[chip].astype(jnp.float32)
    far_arrival(NEAR).wait_recv()
    mixture[...] += far_in[NEAR].astype(jnp.float32)
    far_arrival(FAR + 1).wait_recv()
    mixture[...] += far_in[FAR + 1].astype(jnp.float32)
    hidden_copy(shared_at, 1 - tp).wait_recv()
    own_total = jnp.zeros((rows, 1), jnp.float32)
    for start in range(0, width, tile):
        columns = slice(start, start + tile)
        mixed = mixture[:, columns] + down_product(shared_at, 1 - tp, columns)
        mixture[:, columns] = mixed
        own_total = own_total + jnp.sum(mixed * mixed, axis=-1, keepdims=True)
    square_out[1] = pack(own_total)
    square_copy(1).start()
    loads["out_gain"].wait()
    square_copy(0).wait_send()
    square_copy(1).wait_send()
    for shift in range(1, experts):
        info_copy(shift).wait_send()
    for origin in range(chips):
        gather_copy(origin, 2).wait_send()
        pair_copy(origin).wait_send()

        @pl.when((chip >= origin) & (chip < chips - 1))
        def _(origin=origin):
            gather_copy(origin, 1).wait_send()

        @pl.when((chip <= origin) & (chip > 0))
        def _(origin=origin):
            gather_copy(origin, 0).wait_send()

    for slot in (NEAR, MIDDLE, FAR):
        far_copy(slot).wait_send()

    def drain(k, carry):
        part_copy(k, 0).wait_send()
        part_copy(k, 1).wait_send()
        hidden_copy(k, tp).wait_send()
        return carry

    lax.fori_loop(0, count, drain, 0)
    square_copy(1).wait_recv()
    total = own_total + unpack(square_in[1])
    out_ref[...] = (
        mixture[...] * lax.rsqrt(total / (2 * width) + epsilon) * out_gain_ref[...]
    ).astype(jnp.bfloat16)


def fused(
    chips,
    tokens,
    routes,
    route_weights,
    norm_gain,
    expert_gate,
    expert_up,
    expert_down,
    shared_gate,
    shared_up,
    shared_down,
    out_gain,
):
    rows, width = tokens.shape
    units = shared_gate.shape[1]
    half = units // 2
    count = 2 * chips + 1
    choices = routes.shape[1]
    vmem = pl.BlockSpec(memory_space=pltpu.VMEM)
    hbm = pl.BlockSpec(memory_space=pl.ANY)
    bf16, f32 = jnp.bfloat16, jnp.float32
    dma = pltpu.SemaphoreType.DMA
    return pl.pallas_call(
        functools.partial(fused_kernel, chips),
        out_shape=pltpu.VMEM((rows, width), bf16),
        in_specs=[hbm] * 11,
        out_specs=vmem,
        scratch_shapes=[
            pltpu.VMEM((choices, rows), jnp.int32),
            pltpu.VMEM((choices, rows), f32),
            pltpu.VMEM((1, width), f32),
            pltpu.VMEM((1, width), f32),
            pltpu.VMEM((2, width, units), bf16),
            pltpu.VMEM((2, width, units), bf16),
            pltpu.VMEM((2, units, width), bf16),
            pltpu.VMEM((2 * chips, rows, width), bf16),
            pltpu.VMEM((rows, width), bf16),
            pltpu.VMEM((count, 2, rows, half), bf16),
            pltpu.VMEM((count, 2, rows, half), bf16),
            pltpu.VMEM((count, 2, rows, half), bf16),
            pltpu.VMEM((count, 2, rows, half), bf16),
            pltpu.VMEM((rows, width), f32),
            pltpu.VMEM((3, rows, width), f32),
            pltpu.VMEM((chips, rows, width), bf16),
            pltpu.VMEM((chips, rows, width), bf16),
            pltpu.VMEM((3, rows, width), bf16),
            pltpu.VMEM((4, rows, width), bf16),
            pltpu.VMEM((rows, width), f32),
            pltpu.VMEM((2, 8, rows), f32),
            pltpu.VMEM((2, 8, rows), f32),
            pltpu.VMEM((2 * chips, 8, rows), f32),
            pltpu.VMEM((2 * chips, 8, rows), f32),
            dma((13,)),
            dma((2 * chips,)),
            dma((2 * chips,)),
            dma((2,)),
            dma((2,)),
            dma((chips, 3)),
            dma((chips,)),
            dma((chips,)),
            dma((count, 2)),
            dma((count, 2)),
            dma((count,)),
            dma((count,)),
            dma((chips,)),
            dma((chips,)),
            dma((3,)),
            dma((4,)),
        ],
        compiler_params=pltpu.CompilerParams(
            collective_id=0, has_side_effects=True, vmem_limit_bytes=60 * 1024 * 1024
        ),
    )(
        tokens,
        routes.T,
        route_weights.T,
        norm_gain.reshape(1, -1),
        expert_gate,
        expert_up,
        expert_down,
        shared_gate,
        shared_up,
        shared_down,
        out_gain.reshape(1, -1),
    )


def local_product(source, matrix):
    return jnp.dot(source, matrix, preferred_element_type=jnp.float32)


def per_device(
    tokens,
    routes,
    route_weights,
    norm_gain,
    expert_gate,
    expert_up,
    expert_down,
    shared_gate,
    shared_up,
    shared_down,
    out_gain,
):
    block_width = tokens.shape[1]
    full_width = block_width * lax.axis_size("tp")
    width_index = lax.axis_index("tp")
    full_rows = lax.all_gather(tokens, "tp", axis=1, tiled=True)
    full_float = full_rows.astype(jnp.float32)
    normed_full = (
        full_float
        * lax.rsqrt(jnp.mean(full_float * full_float, axis=-1, keepdims=True) + epsilon)
        * norm_gain
    ).astype(jnp.bfloat16)
    normed_block = lax.dynamic_slice_in_dim(normed_full, width_index * block_width, block_width, 1)
    gate_matrix = expert_gate[0]
    up_matrix = expert_up[0]
    down_matrix = expert_down[0]
    experts = lax.axis_size("ep")
    choose = (routes[:, :, None] == jnp.arange(experts, dtype=jnp.int32)[None, None, :]).astype(
        jnp.float32
    )
    weight_table = jnp.sum(route_weights[:, :, None] * choose, axis=1)
    expert_input = lax.all_gather(normed_block, "ep", axis=0, tiled=True)
    table_all = lax.all_gather(weight_table, "ep", axis=0, tiled=True)
    summed = (
        lax.psum(local_product(expert_input, gate_matrix).astype(jnp.bfloat16), "tp").astype(
            jnp.float32
        ),
        lax.psum(local_product(expert_input, up_matrix).astype(jnp.bfloat16), "tp").astype(
            jnp.float32
        ),
        lax.psum(local_product(normed_block, shared_gate).astype(jnp.bfloat16), "tp").astype(
            jnp.float32
        ),
        lax.psum(local_product(normed_block, shared_up).astype(jnp.bfloat16), "tp").astype(
            jnp.float32
        ),
    )
    routed_hidden = (jax.nn.silu(summed[0]) * summed[1]).astype(jnp.bfloat16)
    shared_hidden = (jax.nn.silu(summed[2]) * summed[3]).astype(jnp.bfloat16)
    expert_rows = local_product(routed_hidden, down_matrix).astype(jnp.bfloat16)
    shared_out = local_product(shared_hidden, shared_down)
    own_expert = lax.axis_index("ep")
    column = lax.dynamic_slice_in_dim(table_all, own_expert, 1, 1)
    routed = lax.psum_scatter(
        (column * expert_rows.astype(jnp.float32)).astype(jnp.bfloat16),
        "ep",
        scatter_dimension=0,
        tiled=True,
    ).astype(jnp.float32)
    mixture = routed + shared_out
    square_sum = lax.psum(jnp.sum(mixture * mixture, axis=-1, keepdims=True), "tp")
    scale = lax.rsqrt(square_sum / full_width + epsilon)
    return (mixture * scale * out_gain).astype(jnp.bfloat16)


def solution(mesh):
    chips = mesh.shape["ep"] // 2
    if mesh.shape["tp"] == 2 and mesh.shape["ep"] == 8:
        body = functools.partial(fused, chips)
    else:
        body = per_device
    return jax.shard_map(
        body,
        mesh=mesh,
        in_specs=(
            P(("grp", "ep"), "tp"),
            P(("grp", "ep"), None),
            P(("grp", "ep"), None),
            P(),
            P("ep", "tp", None),
            P("ep", "tp", None),
            P("ep", None, "tp"),
            P("tp", None),
            P("tp", None),
            P(None, "tp"),
            P("tp"),
        ),
        out_specs=P(("grp", "ep"), "tp"),
        check_vma=False,
    )
```

```python
import functools

import jax
import jax.numpy as jnp
from jax import lax
from jax.experimental import pallas as pl
from jax.experimental.pallas import tpu as pltpu
from jax.sharding import PartitionSpec as P

epsilon = 1e-06
MESH = pl.DeviceIdType.MESH


NEAR, MIDDLE, FAR, SPARE, MIXTURE = range(5)
STEPS = (
    "own",
    (NEAR, 0),
    (MIDDLE, 0),
    (FAR, 0),
    (FAR, 1),
    (MIDDLE, 1),
    (NEAR, 1),
    "other",
)


def pick(index, table):
    value = jnp.int32(table[0])
    for position in range(1, len(table)):
        if table[position] != table[0]:
            value = jnp.where(index == position, jnp.int32(table[position]), value)
    return value


def exclusive_or(a, b, size):
    total, unit = jnp.int32(0), 1
    while unit < size:
        total = total + unit * lax.rem(lax.div(a, unit) + lax.div(b, unit), 2)
        unit *= 2
    return total


def fused_kernel(
    chips,
    tokens_hbm,
    routes_hbm,
    weights_hbm,
    norm_gain_hbm,
    gate_hbm,
    up_hbm,
    down_hbm,
    shared_gate_hbm,
    shared_up_hbm,
    shared_down_hbm,
    out_gain_hbm,
    out_ref,
    routes_ref,
    weights_ref,
    norm_gain_ref,
    out_gain_ref,
    gate,
    up,
    down,
    held,
    source,
    part_out,
    part_in,
    part_own,
    hidden,
    product,
    sums,
    pair_out,
    pair_in,
    far_out,
    far_in,
    square_out,
    square_in,
    info_out,
    info,
    load_sem,
    info_send,
    info_recv,
    square_send,
    square_recv,
    gather_send,
    gather_recv,
    pair_gather_recv,
    part_send,
    part_recv,
    hidden_send,
    hidden_recv,
    pair_send,
    pair_recv,
    far_send,
    far_recv,
):
    rows, width = product.shape
    mixture = sums.at[MIXTURE]
    experts = 2 * chips
    units = gate.shape[2]
    half = units // 2
    count = len(STEPS)
    slots = [step[0] if isinstance(step, tuple) else NEAR for step in STEPS]
    lanes = [
        [side if step == "own" else 1 - side if step == "other" else step[1] if isinstance(step, tuple) else side for step in STEPS]
        for side in range(2)
    ]
    quarter = half // 2
    other_at, shared_at = count - 1, count

    ep = lax.axis_index("ep")
    tp = lax.axis_index("tp")
    chip, core = lax.div(ep, 2), lax.rem(ep, 2)
    other_core = 1 - core
    partner = {"ep": chip * 2 + other_core}
    across = {"tp": 1 - tp}

    away = pl.ds(pl.multiple_of((1 - tp) * half, half), half)
    near = pl.ds(pl.multiple_of(tp * half, half), half)
    features = pl.ds(pl.multiple_of(tp * width, width), width)
    loads = {
        name: pltpu.make_async_copy(source, target, load_sem.at[i])
        for i, (name, source, target) in enumerate(
            [
                ("tokens", tokens_hbm, held.at[ep]),
                ("norm_gain", norm_gain_hbm.at[:, features], norm_gain_ref),
                ("gate_away", gate_hbm.at[0, :, away], gate.at[0, :, away]),
                ("up_away", up_hbm.at[0, :, away], up.at[0, :, away]),
                ("gate_near", gate_hbm.at[0, :, near], gate.at[0, :, near]),
                ("up_near", up_hbm.at[0, :, near], up.at[0, :, near]),
                ("routes", routes_hbm, routes_ref),
                ("weights", weights_hbm, weights_ref),
                ("down", down_hbm.at[0], down.at[0]),
                ("shared_gate", shared_gate_hbm, gate.at[1]),
                ("shared_up", shared_up_hbm, up.at[1]),
                ("shared_down", shared_down_hbm, down.at[1]),
                ("out_gain", out_gain_hbm, out_gain_ref),
            ]
        )
    }
    for load in loads.values():
        load.start()

    barrier = pltpu.get_barrier_semaphore()
    for shift in range(1, experts):
        pl.semaphore_signal(
            barrier,
            inc=1,
            device_id={"ep": lax.rem(ep + shift, experts)},
            device_id_type=MESH,
        )
    pl.semaphore_signal(barrier, inc=1, device_id=across, device_id_type=MESH)

    def remote(source, target, send, recv, device):
        return pltpu.make_async_remote_copy(
            src_ref=source,
            dst_ref=target,
            send_sem=send,
            recv_sem=recv,
            device_id=device,
            device_id_type=MESH,
        )

    def square_copy(which):
        return remote(
            square_out.at[which],
            square_in.at[which],
            square_send.at[which],
            square_recv.at[which],
            across,
        )

    def info_copy(shift):
        return remote(
            info_out.at[shift],
            info.at[ep],
            info_send.at[shift],
            info_recv.at[ep],
            {"ep": lax.rem(ep + shift, experts)},
        )

    def info_arrival(block):
        return remote(info.at[block], info.at[block], info_send.at[0], info_recv.at[block], partner)

    def gather_copy(origin, way):
        slot = held.at[origin * 2 + core]
        device = ({"ep": (chip - 1) * 2 + core}, {"ep": (chip + 1) * 2 + core}, partner)[way]
        recv = (pair_gather_recv if way == 2 else gather_recv).at[origin]
        return remote(slot, slot, gather_send.at[origin, way], recv, device)

    def pair_gather_arrival(origin):
        slot = held.at[origin * 2 + other_core]
        return remote(slot, slot, gather_send.at[origin, 2], pair_gather_recv.at[origin], partner)

    def part_copy(k, which):
        return remote(
            part_out.at[k, which],
            part_in.at[k, which],
            part_send.at[k, which],
            part_recv.at[k, which],
            across,
        )

    def hidden_copy(k, side):
        return remote(
            hidden.at[k, side], hidden.at[k, side], hidden_send.at[k], hidden_recv.at[k], across
        )

    def shared_copy(piece, side):
        slot = hidden.at[shared_at, side, :, piece * quarter : (piece + 1) * quarter]
        at = shared_at + piece
        return remote(slot, slot, hidden_send.at[at], hidden_recv.at[at], across)

    def part_of(piece):
        return pl.ds(piece * (width // 2), width // 2)

    def pair_copy(origin, piece):
        return remote(
            pair_out.at[origin, :, part_of(piece)],
            pair_in.at[origin, :, part_of(piece)],
            pair_send.at[origin, piece],
            pair_recv.at[origin, piece],
            partner,
        )

    beside, opposite, beyond = (exclusive_or(chip, mask, chips) for mask in (1, 2, 3))
    outer = (chip == 0) | (chip == chips - 1)
    inner = jnp.logical_not(outer)

    def origin_of(slot):
        middle, far = jnp.where(outer, opposite, beyond), jnp.where(outer, beyond, opposite)
        return jnp.where(slot == NEAR, beside, jnp.where(slot == MIDDLE, middle, far))

    def far_copy(slot, piece):
        direct = outer | (slot == NEAR)
        place = jnp.where(direct, slot, FAR + 1)
        target = jnp.where(direct, beside, origin_of(slot))
        return remote(
            far_out.at[slot, :, part_of(piece)],
            far_in.at[place, :, part_of(piece)],
            far_send.at[slot, piece],
            far_recv.at[place, piece],
            {"ep": target * 2 + core},
        )

    def far_arrival(place, piece):
        return remote(
            far_out.at[0, :, part_of(piece)],
            far_in.at[place, :, part_of(piece)],
            far_send.at[0, piece],
            far_recv.at[place, piece],
            {"ep": beside * 2 + core},
        )

    def pack(column):
        return jnp.transpose(jnp.broadcast_to(column, (rows, 128)))[:8]

    def unpack(row):
        return jnp.transpose(jnp.broadcast_to(row[:1], (128, rows)))

    def across_lanes(column, lanes):
        return jnp.concatenate([column] * (lanes // 128), axis=1)

    loads["tokens"].wait()
    token_float = held[ep].astype(jnp.float32)
    own_square = jnp.sum(token_float * token_float, axis=-1, keepdims=True)
    square_out[0] = pack(own_square)
    pl.semaphore_wait(barrier, experts)

    def send_outward():
        @pl.when(chip > 0)
        def _():
            gather_copy(chip, 0).start()

        @pl.when(chip < chips - 1)
        def _():
            gather_copy(chip, 1).start()

    pl.when(core == 0)(send_outward)
    gather_copy(chip, 2).start()
    square_copy(0).start()
    loads["norm_gain"].wait()

    def share_info():
        loads["routes"].wait()
        loads["weights"].wait()
        square_copy(0).wait_recv()
        square = square_out[0] + square_in[0]
        scale = lax.rsqrt(square / (2 * width) + epsilon)
        first_row = lax.broadcasted_iota(jnp.int32, scale.shape, 0) == 0
        for shift in range(experts):
            named = routes_ref[...] == lax.rem(ep + shift, experts)
            weight = jnp.sum(jnp.where(named, weights_ref[...], 0.0), axis=0, keepdims=True)
            message = jnp.where(first_row, weight, scale)
            if shift == 0:
                info[ep] = message
            else:
                info_out[shift] = message
                info_copy(shift).start()

    def take(origin):
        gather_copy(origin, 0).wait_recv()
        gather_copy(origin, 2).start()

    def toward_outer(origin):
        @pl.when(chip == 1)
        def _():
            gather_copy(origin, 0).start()

        @pl.when(chip == chips - 2)
        def _():
            gather_copy(origin, 1).start()

    def toward_inner(origin):
        @pl.when(chip < chips // 2)
        def _():
            gather_copy(origin, 1).start()

        @pl.when(chip >= chips // 2)
        def _():
            gather_copy(origin, 0).start()

    def relay(distance):
        @pl.when(chip >= distance)
        def _():
            take(chip - distance)

            @pl.when(chip < chips - 1)
            def _():
                gather_copy(chip - distance, 1).start()

        @pl.when(chip + distance < chips)
        def _():
            take(chip + distance)

            @pl.when(chip > 0)
            def _():
                gather_copy(chip + distance, 0).start()

    def second_lane_before(i):
        @pl.when((i == 4) & inner)
        def _():
            take(beyond)
            toward_outer(beyond)
            toward_outer(chip)

        @pl.when((i >= 4) & (i < 7) & outer)
        def _():
            take(origin_of(pick(i, slots)))

    def second_lane_after(i):
        @pl.when((i == 2) & inner)
        def _():
            take(beside)
            toward_inner(beside)
            toward_inner(chip)

        @pl.when((i == 3) & inner)
        def _():
            take(opposite)
            toward_outer(opposite)

    def locate(k):
        away_from = origin_of(pick(k, slots))
        origin = jnp.where((k == 0) | (k == other_at), chip, away_from)
        lane = jnp.where(core == 0, pick(k, lanes[0]), pick(k, lanes[1]))
        return origin, lane

    def block_of(k):
        origin, lane = locate(k)
        return origin * 2 + lane

    def scaled(block):
        source[...] = (held[block].astype(jnp.float32) * norm_gain_ref[...]).astype(jnp.bfloat16)

    def product_of(matrix, columns):
        return jnp.dot(
            source[...], matrix[columns], preferred_element_type=jnp.float32
        ).astype(jnp.bfloat16)

    def first_stage(k):
        origin, lane = locate(k)
        pl.when((k == 2) & (core == 0) & outer)(functools.partial(relay, 2))
        pl.when((k == 3) & (core == 0))(functools.partial(relay, 3))

        @pl.when(lane != core)
        def _():
            pair_gather_arrival(origin).wait_recv()

        scaled(block_of(k))
        for which, matrix, name in ((0, gate, "gate_away"), (1, up, "up_away")):
            pl.when(k == 0)(loads[name].wait)
            part_out[k, which] = product_of(matrix.at[0], (slice(None), away))
            part_copy(k, which).start()
        for which, matrix, name in ((0, gate, "gate_near"), (1, up, "up_near")):
            pl.when(k == 0)(loads[name].wait)
            part_own[k, which] = product_of(matrix.at[0], (slice(None), near))

    def piece_of(side, piece):
        return pl.ds(pl.multiple_of(side * half + piece * quarter, quarter), quarter)

    def shared_first(piece):
        if piece == 0:
            loads["shared_gate"].wait()
            loads["shared_up"].wait()
        else:
            scaled(ep)
        for side, target in ((1 - tp, part_out), (tp, part_own)):
            columns = (slice(None), piece_of(side, piece))
            for which, matrix in enumerate((gate, up)):
                place = slice(which * quarter, (which + 1) * quarter)
                target[shared_at, piece, :, place] = product_of(matrix.at[1], columns)
            if target is part_out:
                part_copy(shared_at, piece).start()

    def shared_second(piece):
        scale = across_lanes(unpack(info[ep, 1:2]), half)
        part_copy(shared_at, piece).wait_recv()
        total = part_own[shared_at, piece].astype(jnp.float32)
        total = (total + part_in[shared_at, piece].astype(jnp.float32)) * scale
        product_out = jax.nn.silu(total[:, :quarter]) * total[:, quarter:]
        place = slice(piece * quarter, (piece + 1) * quarter)
        hidden[shared_at, tp, :, place] = product_out.astype(jnp.bfloat16)
        shared_copy(piece, tp).start()

    def shared_product(piece, side, columns):
        place = slice(piece * quarter, (piece + 1) * quarter)
        return jnp.dot(
            hidden[shared_at, side, :, place],
            down[1, piece_of(side, piece), columns],
            preferred_element_type=jnp.float32,
        )

    def shared_third():
        loads["shared_down"].wait()

        def own_step(columns):
            mixture[:, columns] += shared_product(0, tp, columns)

        def other_step(columns):
            mixture[:, columns] += shared_product(0, 1 - tp, columns)

        tiles(own_step)
        shared_copy(0, 1 - tp).wait_recv()
        tiles(other_step)

    def second_stage(k):
        block = block_of(k)

        @pl.when(block != ep)
        def _():
            info_arrival(block).wait_recv()

        scale = across_lanes(unpack(info[block, 1:2]), half)
        part_copy(k, 0).wait_recv()
        part_copy(k, 1).wait_recv()
        gate_sum = part_own[k, 0].astype(jnp.float32) + part_in[k, 0].astype(jnp.float32)
        up_sum = part_own[k, 1].astype(jnp.float32) + part_in[k, 1].astype(jnp.float32)
        gate_sum, up_sum = gate_sum * scale, up_sum * scale
        hidden[k, tp] = (jax.nn.silu(gate_sum) * up_sum).astype(jnp.bfloat16)
        hidden_copy(k, tp).start()

    def down_product(k, side, columns):
        rows_of = pl.ds(pl.multiple_of(side * half, half), half)
        return jnp.dot(
            hidden[k, side], down[0, rows_of, columns], preferred_element_type=jnp.float32
        )

    tile = width // 4

    def tiles(step, first=0, last=4):
        def tile_step(i, carry):
            step(pl.ds(pl.multiple_of(i * tile, tile), tile))
            return carry

        lax.fori_loop(first, last, tile_step, 0)

    def third_stage(k):
        origin, lane = locate(k)
        pl.when(k == 0)(loads["down"].wait)

        def own_step(columns):
            product[:, columns] = down_product(k, tp, columns)

        keeper = lane == core
        kept = jnp.where(keeper, jnp.where(k == 0, MIXTURE, pick(k, slots)), SPARE)
        sent = jnp.where(keeper, chips, origin)

        def other_step(columns):
            total = product[:, columns] + down_product(k, 1 - tp, columns)
            weighted = total.astype(jnp.bfloat16).astype(jnp.float32) * scale
            sums[kept, :, columns] = weighted
            pair_out[sent, :, columns] = weighted.astype(jnp.bfloat16)

        tiles(own_step, 0, 4)
        scale = across_lanes(unpack(info[block_of(k), :1]), tile)
        hidden_copy(k, 1 - tp).wait_recv()
        for piece in range(2):
            tiles(other_step, 2 * piece, 2 * piece + 2)

            @pl.when(lane != core)
            def _(piece=piece):
                pair_copy(origin, piece).start()

    def fourth_stage(k):
        origin, lane = locate(k)

        @pl.when((k != 0) & (lane == core))
        def _():
            slot = pick(k, slots)
            direct = outer | (slot == NEAR)
            for piece in range(2):
                columns = part_of(piece)
                pair_copy(origin, piece).wait_recv()
                total = sums[slot, :, columns] + pair_in[origin, :, columns].astype(jnp.float32)
                sums[slot, :, columns] = total
                far_out[slot, :, columns] = total.astype(jnp.bfloat16)

                @pl.when(direct & (k != 1))
                def _(piece=piece):
                    far_copy(slot, piece).start()

    def fifth_stage(k):
        slot = pick(k, slots)
        for piece in range(2):
            columns = part_of(piece)
            far_arrival(slot, piece).wait_recv()
            total = sums[slot, :, columns] + far_in[slot, :, columns].astype(jnp.float32)
            far_out[slot, :, columns] = total.astype(jnp.bfloat16)
            far_copy(slot, piece).start()

    def body(i, carry):
        pl.when(core == 1)(functools.partial(second_lane_before, i))

        @pl.when(i >= 3)
        def _():
            fourth_stage(i - 3)

        @pl.when((i == 6) & (core == 0))
        def _():
            far_copy(NEAR, 0).start()
            far_copy(NEAR, 1).start()

        @pl.when(i == 1)
        def _():
            pl.when(core == 0)(functools.partial(relay, 1))
            second_stage(0)
            pl.when((core == 1) & outer)(functools.partial(toward_inner, chip))

        @pl.when(i < count)
        def _():
            first_stage(i)

        pl.when(core == 1)(functools.partial(second_lane_after, i))

        @pl.when(i == 0)
        def _():
            shared_first(0)
            share_info()

        @pl.when(i == 1)
        def _():
            shared_second(0)

        @pl.when(i == count)
        def _():
            shared_first(1)

        @pl.when(inner & (core == 1) & ((i == 8) | (i == 9)))
        def _():
            fifth_stage(i - 4)

        pl.when((i == 2) & (core == 0) & inner)(functools.partial(relay, 2))

        @pl.when((i >= 2) & (i < count + 1))
        def _():
            second_stage(i - 1)

        @pl.when(inner & (core == 0) & ((i == 6) | (i == 7)))
        def _():
            fifth_stage(i - 4)

        @pl.when(i == count + 1)
        def _():
            shared_second(1)

        @pl.when(i >= 2)
        def _():
            third_stage(i - 2)

        pl.when(i == 3)(shared_third)
        return carry

    lax.fori_loop(0, count + 2, body, 0)

    def shared_own(columns):
        mixture[:, columns] += shared_product(1, tp, columns)

    tiles(shared_own)
    for piece in range(2):
        pair_copy(chip, piece).wait_recv()
        mixture[:, part_of(piece)] += pair_in[chip, :, part_of(piece)].astype(jnp.float32)
    for place in (FAR + 1, NEAR):
        for piece in range(2):
            columns = part_of(piece)
            far_arrival(place, piece).wait_recv()
            mixture[:, columns] += far_in[place, :, columns].astype(jnp.float32)
    shared_copy(1, 1 - tp).wait_recv()
    own_total = jnp.zeros((rows, 1), jnp.float32)
    for start in range(0, width, tile):
        columns = slice(start, start + tile)
        mixed = mixture[:, columns] + shared_product(1, 1 - tp, columns)
        mixture[:, columns] = mixed
        own_total = own_total + jnp.sum(mixed * mixed, axis=-1, keepdims=True)
    square_out[1] = pack(own_total)
    square_copy(1).start()
    loads["out_gain"].wait()
    mixture[...] *= out_gain_ref[...]
    square_copy(0).wait_send()
    square_copy(1).wait_send()
    for shift in range(1, experts):
        info_copy(shift).wait_send()
    for origin in range(chips):
        gather_copy(origin, 2).wait_send()
        pair_copy(origin, 0).wait_send()
        pair_copy(origin, 1).wait_send()

        @pl.when((chip >= origin) & (chip < chips - 1))
        def _(origin=origin):
            gather_copy(origin, 1).wait_send()

        @pl.when((chip <= origin) & (chip > 0))
        def _(origin=origin):
            gather_copy(origin, 0).wait_send()

    for slot in (NEAR, MIDDLE, FAR):
        far_copy(slot, 0).wait_send()
        far_copy(slot, 1).wait_send()

    def drain(k, carry):
        part_copy(k, 0).wait_send()
        part_copy(k, 1).wait_send()
        hidden_copy(k, tp).wait_send()
        return carry

    lax.fori_loop(0, count, drain, 0)
    for piece in range(2):
        part_copy(shared_at, piece).wait_send()
        shared_copy(piece, tp).wait_send()

    square_copy(1).wait_recv()
    scale = lax.rsqrt((own_total + unpack(square_in[1])) / (2 * width) + epsilon)
    out_ref[...] = (mixture[...] * across_lanes(scale, width)).astype(jnp.bfloat16)


def fused(
    chips,
    tokens,
    routes,
    route_weights,
    norm_gain,
    expert_gate,
    expert_up,
    expert_down,
    shared_gate,
    shared_up,
    shared_down,
    out_gain,
):
    rows, width = tokens.shape
    units = shared_gate.shape[1]
    half = units // 2
    count = 2 * chips + 1
    choices = routes.shape[1]
    vmem = pl.BlockSpec(memory_space=pltpu.VMEM)
    hbm = pl.BlockSpec(memory_space=pl.ANY)
    bf16, f32 = jnp.bfloat16, jnp.float32
    dma = pltpu.SemaphoreType.DMA
    return pl.pallas_call(
        functools.partial(fused_kernel, chips),
        out_shape=pltpu.VMEM((rows, width), bf16),
        in_specs=[hbm] * 11,
        out_specs=vmem,
        scratch_shapes=[
            pltpu.VMEM((choices, rows), jnp.int32),
            pltpu.VMEM((choices, rows), f32),
            pltpu.VMEM((1, width), f32),
            pltpu.VMEM((1, width), f32),
            pltpu.VMEM((2, width, units), bf16),
            pltpu.VMEM((2, width, units), bf16),
            pltpu.VMEM((2, units, width), bf16),
            pltpu.VMEM((2 * chips, rows, width), bf16),
            pltpu.VMEM((rows, width), bf16),
            pltpu.VMEM((count, 2, rows, half), bf16),
            pltpu.VMEM((count, 2, rows, half), bf16),
            pltpu.VMEM((count, 2, rows, half), bf16),
            pltpu.VMEM((count, 2, rows, half), bf16),
            pltpu.VMEM((rows, width), f32),
            pltpu.VMEM((5, rows, width), f32),
            pltpu.VMEM((chips + 1, rows, width), bf16),
            pltpu.VMEM((chips, rows, width), bf16),
            pltpu.VMEM((3, rows, width), bf16),
            pltpu.VMEM((4, rows, width), bf16),
            pltpu.VMEM((2, 8, rows), f32),
            pltpu.VMEM((2, 8, rows), f32),
            pltpu.VMEM((2 * chips, 8, rows), f32),
            pltpu.VMEM((2 * chips, 8, rows), f32),
            dma((13,)),
            dma((2 * chips,)),
            dma((2 * chips,)),
            dma((2,)),
            dma((2,)),
            dma((chips, 3)),
            dma((chips,)),
            dma((chips,)),
            dma((count, 2)),
            dma((count, 2)),
            dma((count + 1,)),
            dma((count + 1,)),
            dma((chips, 2)),
            dma((chips, 2)),
            dma((3, 2)),
            dma((4, 2)),
        ],
        compiler_params=pltpu.CompilerParams(
            collective_id=0, has_side_effects=True, vmem_limit_bytes=60 * 1024 * 1024
        ),
    )(
        tokens,
        routes.T,
        route_weights.T,
        norm_gain.reshape(1, -1),
        expert_gate,
        expert_up,
        expert_down,
        shared_gate,
        shared_up,
        shared_down,
        out_gain.reshape(1, -1),
    )


def local_product(source, matrix):
    return jnp.dot(source, matrix, preferred_element_type=jnp.float32)


def per_device(
    tokens,
    routes,
    route_weights,
    norm_gain,
    expert_gate,
    expert_up,
    expert_down,
    shared_gate,
    shared_up,
    shared_down,
    out_gain,
):
    block_width = tokens.shape[1]
    full_width = block_width * lax.axis_size("tp")
    width_index = lax.axis_index("tp")
    full_rows = lax.all_gather(tokens, "tp", axis=1, tiled=True)
    full_float = full_rows.astype(jnp.float32)
    normed_full = (
        full_float
        * lax.rsqrt(jnp.mean(full_float * full_float, axis=-1, keepdims=True) + epsilon)
        * norm_gain
    ).astype(jnp.bfloat16)
    normed_block = lax.dynamic_slice_in_dim(normed_full, width_index * block_width, block_width, 1)
    gate_matrix = expert_gate[0]
    up_matrix = expert_up[0]
    down_matrix = expert_down[0]
    experts = lax.axis_size("ep")
    choose = (routes[:, :, None] == jnp.arange(experts, dtype=jnp.int32)[None, None, :]).astype(
        jnp.float32
    )
    weight_table = jnp.sum(route_weights[:, :, None] * choose, axis=1)
    expert_input = lax.all_gather(normed_block, "ep", axis=0, tiled=True)
    table_all = lax.all_gather(weight_table, "ep", axis=0, tiled=True)
    summed = (
        lax.psum(local_product(expert_input, gate_matrix).astype(jnp.bfloat16), "tp").astype(
            jnp.float32
        ),
        lax.psum(local_product(expert_input, up_matrix).astype(jnp.bfloat16), "tp").astype(
            jnp.float32
        ),
        lax.psum(local_product(normed_block, shared_gate).astype(jnp.bfloat16), "tp").astype(
            jnp.float32
        ),
        lax.psum(local_product(normed_block, shared_up).astype(jnp.bfloat16), "tp").astype(
            jnp.float32
        ),
    )
    routed_hidden = (jax.nn.silu(summed[0]) * summed[1]).astype(jnp.bfloat16)
    shared_hidden = (jax.nn.silu(summed[2]) * summed[3]).astype(jnp.bfloat16)
    expert_rows = local_product(routed_hidden, down_matrix).astype(jnp.bfloat16)
    shared_out = local_product(shared_hidden, shared_down)
    own_expert = lax.axis_index("ep")
    column = lax.dynamic_slice_in_dim(table_all, own_expert, 1, 1)
    routed = lax.psum_scatter(
        (column * expert_rows.astype(jnp.float32)).astype(jnp.bfloat16),
        "ep",
        scatter_dimension=0,
        tiled=True,
    ).astype(jnp.float32)
    mixture = routed + shared_out
    square_sum = lax.psum(jnp.sum(mixture * mixture, axis=-1, keepdims=True), "tp")
    scale = lax.rsqrt(square_sum / full_width + epsilon)
    return (mixture * scale * out_gain).astype(jnp.bfloat16)


def solution(mesh):
    chips = mesh.shape["ep"] // 2
    if mesh.shape["tp"] == 2 and mesh.shape["ep"] == 8:
        body = functools.partial(fused, chips)
    else:
        body = per_device
    return jax.shard_map(
        body,
        mesh=mesh,
        in_specs=(
            P(("grp", "ep"), "tp"),
            P(("grp", "ep"), None),
            P(("grp", "ep"), None),
            P(),
            P("ep", "tp", None),
            P("ep", "tp", None),
            P("ep", None, "tp"),
            P("tp", None),
            P("tp", None),
            P(None, "tp"),
            P("tp"),
        ),
        out_specs=P(("grp", "ep"), "tp"),
        check_vma=False,
    )
```

```python
import functools

import jax
import jax.numpy as jnp
from jax import lax
from jax.experimental import pallas as pl
from jax.experimental.pallas import tpu as pltpu
from jax.sharding import PartitionSpec as P

epsilon = 1e-06
MESH = pl.DeviceIdType.MESH


NEAR, MIDDLE, FAR, SPARE, MIXTURE = range(5)
STEPS = (
    "own",
    (NEAR, 0),
    (MIDDLE, 0),
    (FAR, 0),
    (FAR, 1),
    (MIDDLE, 1),
    (NEAR, 1),
    "other",
)


def pick(index, table):
    value = jnp.int32(table[0])
    for position in range(1, len(table)):
        if table[position] != table[0]:
            value = jnp.where(index == position, jnp.int32(table[position]), value)
    return value


def exclusive_or(a, b, size):
    total, unit = jnp.int32(0), 1
    while unit < size:
        total = total + unit * lax.rem(lax.div(a, unit) + lax.div(b, unit), 2)
        unit *= 2
    return total


def fused_kernel(
    chips,
    tokens_hbm,
    routes_hbm,
    weights_hbm,
    norm_gain_hbm,
    gate_hbm,
    up_hbm,
    down_hbm,
    shared_gate_hbm,
    shared_up_hbm,
    shared_down_hbm,
    out_gain_hbm,
    out_ref,
    routes_ref,
    weights_ref,
    norm_gain_ref,
    out_gain_ref,
    gate,
    up,
    down,
    held,
    source,
    part_out,
    part_in,
    part_own,
    hidden,
    product,
    sums,
    pair_out,
    pair_in,
    far_out,
    far_in,
    square_out,
    square_in,
    info_out,
    info,
    load_sem,
    info_send,
    info_recv,
    square_send,
    square_recv,
    gather_send,
    gather_recv,
    pair_gather_recv,
    part_send,
    part_recv,
    hidden_send,
    hidden_recv,
    pair_send,
    pair_recv,
    far_send,
    far_recv,
):
    rows, width = product.shape
    mixture = sums.at[MIXTURE]
    experts = 2 * chips
    units = gate.shape[2]
    half = units // 2
    count = len(STEPS)
    slots = [step[0] if isinstance(step, tuple) else NEAR for step in STEPS]
    lanes = [
        [side if step == "own" else 1 - side if step == "other" else step[1] if isinstance(step, tuple) else side for step in STEPS]
        for side in range(2)
    ]
    quarter = half // 2
    other_at, shared_at = count - 1, count

    ep = lax.axis_index("ep")
    tp = lax.axis_index("tp")
    chip, core = lax.div(ep, 2), lax.rem(ep, 2)
    other_core = 1 - core
    partner = {"ep": chip * 2 + other_core}
    across = {"tp": 1 - tp}

    away = pl.ds(pl.multiple_of((1 - tp) * half, half), half)
    near = pl.ds(pl.multiple_of(tp * half, half), half)
    features = pl.ds(pl.multiple_of(tp * width, width), width)
    groups = [
        [(tokens_hbm, held.at[ep])],
        [(norm_gain_hbm.at[:, features], norm_gain_ref)],
        [(gate_hbm.at[0, :, away], gate.at[0, :, away])],
        [(up_hbm.at[0, :, away], up.at[0, :, away])],
        [
            (gate_hbm.at[0, :, near], gate.at[0, :, near]),
            (up_hbm.at[0, :, near], up.at[0, :, near]),
        ],
        [(routes_hbm, routes_ref), (weights_hbm, weights_ref)],
        [(shared_gate_hbm, gate.at[1]), (shared_up_hbm, up.at[1])],
        [(down_hbm.at[0], down.at[0]), (shared_down_hbm, down.at[1])],
        [(out_gain_hbm, out_gain_ref)],
    ]
    wholes = [held.at[ep], norm_gain_ref, gate.at[0, :, away], up.at[0, :, away]]
    wholes += [gate.at[0], info.at[0], gate, down, out_gain_ref]
    names = ["tokens", "norm_gain", "gate_away", "up_away", "near", "table"]
    names += ["shared_in", "down", "out_gain"]

    loads = {
        name: pltpu.make_async_copy(whole, whole, load_sem.at[i])
        for i, (name, whole) in enumerate(zip(names, wholes))
    }
    for i, group in enumerate(groups):
        for load_from, load_to in group:
            pltpu.make_async_copy(load_from, load_to, load_sem.at[i]).start()

    barrier = pltpu.get_barrier_semaphore()
    for shift in range(1, experts):
        pl.semaphore_signal(
            barrier,
            inc=1,
            device_id={"ep": lax.rem(ep + shift, experts)},
            device_id_type=MESH,
        )
    pl.semaphore_signal(barrier, inc=1, device_id=across, device_id_type=MESH)

    def remote(source, target, send, recv, device):
        return pltpu.make_async_remote_copy(
            src_ref=source,
            dst_ref=target,
            send_sem=send,
            recv_sem=recv,
            device_id=device,
            device_id_type=MESH,
        )

    def square_copy(which):
        return remote(
            square_out.at[which],
            square_in.at[which],
            square_send.at[which],
            square_recv.at[which],
            across,
        )

    def info_copy(shift):
        return remote(
            info_out.at[shift],
            info.at[ep],
            info_send.at[0],
            info_recv.at[0],
            {"ep": lax.rem(ep + shift, experts)},
        )

    def info_all():
        return remote(
            info_out.at[1:], info_out.at[1:], info_send.at[0], info_recv.at[0], partner
        )

    def gather_copy(origin, way):
        slot = held.at[origin * 2 + core]
        device = ({"ep": (chip - 1) * 2 + core}, {"ep": (chip + 1) * 2 + core}, partner)[way]
        recv = (pair_gather_recv if way == 2 else gather_recv).at[origin]
        return remote(slot, slot, gather_send.at[way // 2], recv, device)

    def pair_gather_arrival(origin):
        slot = held.at[origin * 2 + other_core]
        return remote(slot, slot, gather_send.at[1], pair_gather_recv.at[origin], partner)

    def part_copy(k, which):
        place = lax.rem(k, 3)
        return remote(
            part_out.at[k, which],
            part_in.at[k, which],
            part_send.at[0],
            part_recv.at[place],
            across,
        )

    def part_arrival(k):
        place = lax.rem(k, 3)
        return remote(
            part_out.at[k], part_in.at[k], part_send.at[0], part_recv.at[place], across
        )

    def shared_part_copy(piece):
        return remote(
            part_out.at[shared_at, piece],
            part_in.at[shared_at, piece],
            part_send.at[0],
            part_recv.at[3 + piece],
            across,
        )

    def hidden_copy(k, side):
        slot = hidden.at[k, side]
        return remote(slot, slot, hidden_send.at[0], hidden_recv.at[lax.rem(k, 4)], across)

    def shared_copy(piece, side):
        slot = hidden.at[shared_at, side, :, piece * quarter : (piece + 1) * quarter]
        return remote(slot, slot, hidden_send.at[0], hidden_recv.at[4 + piece], across)

    def part_of(piece):
        return pl.ds(piece * (width // 2), width // 2)

    def pair_copy(origin, piece):
        return remote(
            pair_out.at[origin, :, part_of(piece)],
            pair_in.at[origin, :, part_of(piece)],
            pair_send.at[0],
            pair_recv.at[origin, piece],
            partner,
        )

    beside, opposite, beyond = (exclusive_or(chip, mask, chips) for mask in (1, 2, 3))
    outer = (chip == 0) | (chip == chips - 1)
    inner = jnp.logical_not(outer)

    def origin_of(slot):
        middle, far = jnp.where(outer, opposite, beyond), jnp.where(outer, beyond, opposite)
        return jnp.where(slot == NEAR, beside, jnp.where(slot == MIDDLE, middle, far))

    def far_copy(slot, piece):
        direct = outer | (slot == NEAR)
        place = jnp.where(direct, slot, FAR + 1)
        target = jnp.where(direct, beside, origin_of(slot))
        return remote(
            far_out.at[slot, :, part_of(piece)],
            far_in.at[place, :, part_of(piece)],
            far_send.at[0],
            far_recv.at[place, piece],
            {"ep": target * 2 + core},
        )

    def far_arrival(place, piece):
        return remote(
            far_out.at[0, :, part_of(piece)],
            far_in.at[place, :, part_of(piece)],
            far_send.at[0],
            far_recv.at[place, piece],
            {"ep": beside * 2 + core},
        )

    def pack(column):
        return jnp.transpose(jnp.broadcast_to(column, (rows, 128)))[:8]

    def unpack(row):
        return jnp.transpose(jnp.broadcast_to(row[:1], (128, rows)))

    def across_lanes(column, lanes):
        return jnp.concatenate([column] * (lanes // 128), axis=1)

    loads["tokens"].wait()
    token_float = held[ep].astype(jnp.float32)
    own_square = jnp.sum(token_float * token_float, axis=-1, keepdims=True)
    square_out[0] = pack(own_square)
    pl.semaphore_wait(barrier, experts)

    def send_outward():
        @pl.when(chip > 0)
        def _():
            gather_copy(chip, 0).start()

        @pl.when(chip < chips - 1)
        def _():
            gather_copy(chip, 1).start()

    pl.when(core == 0)(send_outward)
    gather_copy(chip, 2).start()
    square_copy(0).start()
    loads["norm_gain"].wait()

    def share_info():
        loads["table"].wait()
        square_copy(0).wait_recv()
        square = square_out[0] + square_in[0]
        scale = lax.rsqrt(square / (2 * width) + epsilon)
        first_row = lax.broadcasted_iota(jnp.int32, scale.shape, 0) == 0
        for shift in range(experts):
            named = routes_ref[...] == lax.rem(ep + shift, experts)
            weight = jnp.sum(jnp.where(named, weights_ref[...], 0.0), axis=0, keepdims=True)
            message = jnp.where(first_row, weight, scale)
            if shift == 0:
                info[ep] = message
            else:
                info_out[shift] = message
                info_copy(shift).start()

    def take(origin):
        gather_copy(origin, 0).wait_recv()
        gather_copy(origin, 2).start()

    def toward_outer(origin):
        @pl.when(chip == 1)
        def _():
            gather_copy(origin, 0).start()

        @pl.when(chip == chips - 2)
        def _():
            gather_copy(origin, 1).start()

    def toward_inner(origin):
        @pl.when(chip < chips // 2)
        def _():
            gather_copy(origin, 1).start()

        @pl.when(chip >= chips // 2)
        def _():
            gather_copy(origin, 0).start()

    def relay(distance):
        @pl.when(chip >= distance)
        def _():
            take(chip - distance)

            @pl.when(chip < chips - 1)
            def _():
                gather_copy(chip - distance, 1).start()

        @pl.when(chip + distance < chips)
        def _():
            take(chip + distance)

            @pl.when(chip > 0)
            def _():
                gather_copy(chip + distance, 0).start()

    def second_lane_before(i):
        @pl.when((i == 4) & inner)
        def _():
            take(beyond)
            toward_outer(beyond)
            toward_outer(chip)

        @pl.when((i >= 4) & (i < 7) & outer)
        def _():
            take(origin_of(pick(i, slots)))

    def second_lane_after(i):
        @pl.when((i == 2) & inner)
        def _():
            take(beside)
            toward_inner(beside)
            toward_inner(chip)

        @pl.when((i == 3) & inner)
        def _():
            take(opposite)
            toward_outer(opposite)

    def locate(k):
        away_from = origin_of(pick(k, slots))
        origin = jnp.where((k == 0) | (k == other_at), chip, away_from)
        lane = jnp.where(core == 0, pick(k, lanes[0]), pick(k, lanes[1]))
        return origin, lane

    def block_of(k):
        origin, lane = locate(k)
        return origin * 2 + lane

    def scaled(block):
        source[...] = (held[block].astype(jnp.float32) * norm_gain_ref[...]).astype(jnp.bfloat16)

    def product_of(matrix, columns):
        return jnp.dot(
            source[...], matrix[columns], preferred_element_type=jnp.float32
        ).astype(jnp.bfloat16)

    def first_stage(k):
        origin, lane = locate(k)
        pl.when((k == 2) & (core == 0) & outer)(functools.partial(relay, 2))
        pl.when((k == 3) & (core == 0))(functools.partial(relay, 3))

        @pl.when(lane != core)
        def _():
            pair_gather_arrival(origin).wait_recv()

        scaled(block_of(k))
        for which, matrix, name in ((0, gate, "gate_away"), (1, up, "up_away")):
            pl.when(k == 0)(loads[name].wait)
            part_out[k, which] = product_of(matrix.at[0], (slice(None), away))
            part_copy(k, which).start()
        pl.when(k == 0)(loads["near"].wait)
        for which, matrix in enumerate((gate, up)):
            part_own[k, which] = product_of(matrix.at[0], (slice(None), near))

    def piece_of(side, piece):
        return pl.ds(pl.multiple_of(side * half + piece * quarter, quarter), quarter)

    def shared_first(piece):
        if piece == 0:
            loads["shared_in"].wait()
        else:
            scaled(ep)
        for side, target in ((1 - tp, part_out), (tp, part_own)):
            columns = (slice(None), piece_of(side, piece))
            for which, matrix in enumerate((gate, up)):
                place = slice(which * quarter, (which + 1) * quarter)
                target[shared_at, piece, :, place] = product_of(matrix.at[1], columns)
            if target is part_out:
                shared_part_copy(piece).start()

    def shared_second(piece):
        scale = across_lanes(unpack(info[ep, 1:2]), half)
        shared_part_copy(piece).wait_recv()
        total = part_own[shared_at, piece].astype(jnp.float32)
        total = (total + part_in[shared_at, piece].astype(jnp.float32)) * scale
        product_out = jax.nn.silu(total[:, :quarter]) * total[:, quarter:]
        place = slice(piece * quarter, (piece + 1) * quarter)
        hidden[shared_at, tp, :, place] = product_out.astype(jnp.bfloat16)
        shared_copy(piece, tp).start()

    def shared_product(piece, side, columns):
        place = slice(piece * quarter, (piece + 1) * quarter)
        return jnp.dot(
            hidden[shared_at, side, :, place],
            down[1, piece_of(side, piece), columns],
            preferred_element_type=jnp.float32,
        )

    def shared_third():
        def own_step(columns):
            mixture[:, columns] += shared_product(0, tp, columns)

        def other_step(columns):
            mixture[:, columns] += shared_product(0, 1 - tp, columns)

        tiles(own_step)
        shared_copy(0, 1 - tp).wait_recv()
        tiles(other_step)

    def second_stage(k):
        block = block_of(k)

        pl.when(k == 1)(info_all().wait_recv)
        scale = across_lanes(unpack(info[block, 1:2]), half)
        part_arrival(k).wait_recv()
        gate_sum = part_own[k, 0].astype(jnp.float32) + part_in[k, 0].astype(jnp.float32)
        up_sum = part_own[k, 1].astype(jnp.float32) + part_in[k, 1].astype(jnp.float32)
        gate_sum, up_sum = gate_sum * scale, up_sum * scale
        hidden[k, tp] = (jax.nn.silu(gate_sum) * up_sum).astype(jnp.bfloat16)
        hidden_copy(k, tp).start()

    def down_product(k, side, columns):
        rows_of = pl.ds(pl.multiple_of(side * half, half), half)
        return jnp.dot(
            hidden[k, side], down[0, rows_of, columns], preferred_element_type=jnp.float32
        )

    tile = width // 4

    def tiles(step, first=0, last=4):
        def tile_step(i, carry):
            step(pl.ds(pl.multiple_of(i * tile, tile), tile))
            return carry

        lax.fori_loop(first, last, tile_step, 0)

    def third_stage(k):
        origin, lane = locate(k)
        pl.when(k == 0)(loads["down"].wait)

        def own_step(columns):
            product[:, columns] = down_product(k, tp, columns)

        keeper = lane == core
        kept = jnp.where(keeper, jnp.where(k == 0, MIXTURE, pick(k, slots)), SPARE)
        sent = jnp.where(keeper, chips, origin)

        def other_step(columns):
            total = product[:, columns] + down_product(k, 1 - tp, columns)
            weighted = total.astype(jnp.bfloat16).astype(jnp.float32) * scale
            sums[kept, :, columns] = weighted
            pair_out[sent, :, columns] = weighted.astype(jnp.bfloat16)

        tiles(own_step, 0, 4)
        scale = across_lanes(unpack(info[block_of(k), :1]), tile)
        hidden_copy(k, 1 - tp).wait_recv()
        for piece in range(2):
            tiles(other_step, 2 * piece, 2 * piece + 2)

            @pl.when(lane != core)
            def _(piece=piece):
                pair_copy(origin, piece).start()

    def fourth_stage(k):
        origin, lane = locate(k)

        @pl.when((k != 0) & (lane == core))
        def _():
            slot = pick(k, slots)
            direct = outer | (slot == NEAR)
            for piece in range(2):
                columns = part_of(piece)
                pair_copy(origin, piece).wait_recv()
                total = sums[slot, :, columns] + pair_in[origin, :, columns].astype(jnp.float32)
                sums[slot, :, columns] = total
                far_out[slot, :, columns] = total.astype(jnp.bfloat16)

                @pl.when(direct & (k != 1))
                def _(piece=piece):
                    far_copy(slot, piece).start()

    def fifth_stage(k):
        slot = pick(k, slots)
        for piece in range(2):
            columns = part_of(piece)
            far_arrival(slot, piece).wait_recv()
            total = sums[slot, :, columns] + far_in[slot, :, columns].astype(jnp.float32)
            far_out[slot, :, columns] = total.astype(jnp.bfloat16)
            far_copy(slot, piece).start()

    def body(i, carry):
        pl.when(core == 1)(functools.partial(second_lane_before, i))

        @pl.when(i >= 3)
        def _():
            fourth_stage(i - 3)

        @pl.when((i == 6) & (core == 0))
        def _():
            far_copy(NEAR, 0).start()
            far_copy(NEAR, 1).start()

        @pl.when(i == 1)
        def _():
            pl.when(core == 0)(functools.partial(relay, 1))
            second_stage(0)
            pl.when((core == 1) & outer)(functools.partial(toward_inner, chip))

        @pl.when(i < count)
        def _():
            first_stage(i)

        pl.when(core == 1)(functools.partial(second_lane_after, i))

        @pl.when(i == 0)
        def _():
            shared_first(0)
            share_info()

        @pl.when(i == 1)
        def _():
            shared_second(0)

        @pl.when(i == count)
        def _():
            shared_first(1)

        @pl.when(inner & (core == 1) & ((i == 8) | (i == 9)))
        def _():
            fifth_stage(i - 4)

        pl.when((i == 2) & (core == 0) & inner)(functools.partial(relay, 2))

        @pl.when((i >= 2) & (i < count + 1))
        def _():
            second_stage(i - 1)

        @pl.when(inner & (core == 0) & ((i == 6) | (i == 7)))
        def _():
            fifth_stage(i - 4)

        @pl.when(i == count + 1)
        def _():
            shared_second(1)

        @pl.when(i >= 2)
        def _():
            third_stage(i - 2)

        pl.when(i == 3)(shared_third)
        return carry

    lax.fori_loop(0, count + 2, body, 0)

    def shared_own(columns):
        mixture[:, columns] += shared_product(1, tp, columns)

    tiles(shared_own)
    for piece in range(2):
        pair_copy(chip, piece).wait_recv()
        mixture[:, part_of(piece)] += pair_in[chip, :, part_of(piece)].astype(jnp.float32)
    for place in (FAR + 1, NEAR):
        for piece in range(2):
            columns = part_of(piece)
            far_arrival(place, piece).wait_recv()
            mixture[:, columns] += far_in[place, :, columns].astype(jnp.float32)
    shared_copy(1, 1 - tp).wait_recv()
    own_total = jnp.zeros((rows, 1), jnp.float32)
    for start in range(0, width, tile):
        columns = slice(start, start + tile)
        mixed = mixture[:, columns] + shared_product(1, 1 - tp, columns)
        mixture[:, columns] = mixed
        own_total = own_total + jnp.sum(mixed * mixed, axis=-1, keepdims=True)
    square_out[1] = pack(own_total)
    square_copy(1).start()
    loads["out_gain"].wait()
    mixture[...] *= out_gain_ref[...]
    square_copy(0).wait_send()
    square_copy(1).wait_send()
    info_all().wait_send()

    def sent(whole, sem):
        pltpu.make_async_copy(whole, whole, sem.at[0]).wait()

    @pl.when(outer)
    def _():
        pltpu.make_async_copy(held.at[0], held.at[0], gather_send.at[0]).wait()

    @pl.when(inner)
    def _():
        several = held.at[: chips + 1]
        pltpu.make_async_copy(several, several, gather_send.at[0]).wait()

    pltpu.make_async_copy(held.at[:chips], held.at[:chips], gather_send.at[1]).wait()
    sent(part_out, part_send)
    sent(part_out.at[:, 0], hidden_send)
    sent(pair_in, pair_send)
    sent(far_out, far_send)
    square_copy(1).wait_recv()
    scale = lax.rsqrt((own_total + unpack(square_in[1])) / (2 * width) + epsilon)
    out_ref[...] = (mixture[...] * across_lanes(scale, width)).astype(jnp.bfloat16)


def fused(
    chips,
    tokens,
    routes,
    route_weights,
    norm_gain,
    expert_gate,
    expert_up,
    expert_down,
    shared_gate,
    shared_up,
    shared_down,
    out_gain,
):
    rows, width = tokens.shape
    units = shared_gate.shape[1]
    half = units // 2
    count = 2 * chips + 1
    choices = routes.shape[1]
    vmem = pl.BlockSpec(memory_space=pltpu.VMEM)
    hbm = pl.BlockSpec(memory_space=pl.ANY)
    bf16, f32 = jnp.bfloat16, jnp.float32
    dma = pltpu.SemaphoreType.DMA
    return pl.pallas_call(
        functools.partial(fused_kernel, chips),
        out_shape=pltpu.VMEM((rows, width), bf16),
        in_specs=[hbm] * 11,
        out_specs=vmem,
        scratch_shapes=[
            pltpu.VMEM((choices, rows), jnp.int32),
            pltpu.VMEM((choices, rows), f32),
            pltpu.VMEM((1, width), f32),
            pltpu.VMEM((1, width), f32),
            pltpu.VMEM((2, width, units), bf16),
            pltpu.VMEM((2, width, units), bf16),
            pltpu.VMEM((2, units, width), bf16),
            pltpu.VMEM((2 * chips, rows, width), bf16),
            pltpu.VMEM((rows, width), bf16),
            pltpu.VMEM((count, 2, rows, half), bf16),
            pltpu.VMEM((count, 2, rows, half), bf16),
            pltpu.VMEM((count, 2, rows, half), bf16),
            pltpu.VMEM((count, 2, rows, half), bf16),
            pltpu.VMEM((rows, width), f32),
            pltpu.VMEM((5, rows, width), f32),
            pltpu.VMEM((chips + 1, rows, width), bf16),
            pltpu.VMEM((chips, rows, width), bf16),
            pltpu.VMEM((3, rows, width), bf16),
            pltpu.VMEM((4, rows, width), bf16),
            pltpu.VMEM((2, 8, rows), f32),
            pltpu.VMEM((2, 8, rows), f32),
            pltpu.VMEM((2 * chips, 8, rows), f32),
            pltpu.VMEM((2 * chips, 8, rows), f32),
            dma((9,)),
            dma((1,)),
            dma((1,)),
            dma((2,)),
            dma((2,)),
            dma((2,)),
            dma((chips,)),
            dma((chips,)),
            dma((1,)),
            dma((5,)),
            dma((1,)),
            dma((6,)),
            dma((1,)),
            dma((chips, 2)),
            dma((1,)),
            dma((4, 2)),
        ],
        compiler_params=pltpu.CompilerParams(
            collective_id=0, has_side_effects=True, vmem_limit_bytes=60 * 1024 * 1024
        ),
    )(
        tokens,
        routes.T,
        route_weights.T,
        norm_gain.reshape(1, -1),
        expert_gate,
        expert_up,
        expert_down,
        shared_gate,
        shared_up,
        shared_down,
        out_gain.reshape(1, -1),
    )


def local_product(source, matrix):
    return jnp.dot(source, matrix, preferred_element_type=jnp.float32)


def per_device(
    tokens,
    routes,
    route_weights,
    norm_gain,
    expert_gate,
    expert_up,
    expert_down,
    shared_gate,
    shared_up,
    shared_down,
    out_gain,
):
    block_width = tokens.shape[1]
    full_width = block_width * lax.axis_size("tp")
    width_index = lax.axis_index("tp")
    full_rows = lax.all_gather(tokens, "tp", axis=1, tiled=True)
    full_float = full_rows.astype(jnp.float32)
    normed_full = (
        full_float
        * lax.rsqrt(jnp.mean(full_float * full_float, axis=-1, keepdims=True) + epsilon)
        * norm_gain
    ).astype(jnp.bfloat16)
    normed_block = lax.dynamic_slice_in_dim(normed_full, width_index * block_width, block_width, 1)
    gate_matrix = expert_gate[0]
    up_matrix = expert_up[0]
    down_matrix = expert_down[0]
    experts = lax.axis_size("ep")
    choose = (routes[:, :, None] == jnp.arange(experts, dtype=jnp.int32)[None, None, :]).astype(
        jnp.float32
    )
    weight_table = jnp.sum(route_weights[:, :, None] * choose, axis=1)
    expert_input = lax.all_gather(normed_block, "ep", axis=0, tiled=True)
    table_all = lax.all_gather(weight_table, "ep", axis=0, tiled=True)
    summed = (
        lax.psum(local_product(expert_input, gate_matrix).astype(jnp.bfloat16), "tp").astype(
            jnp.float32
        ),
        lax.psum(local_product(expert_input, up_matrix).astype(jnp.bfloat16), "tp").astype(
            jnp.float32
        ),
        lax.psum(local_product(normed_block, shared_gate).astype(jnp.bfloat16), "tp").astype(
            jnp.float32
        ),
        lax.psum(local_product(normed_block, shared_up).astype(jnp.bfloat16), "tp").astype(
            jnp.float32
        ),
    )
    routed_hidden = (jax.nn.silu(summed[0]) * summed[1]).astype(jnp.bfloat16)
    shared_hidden = (jax.nn.silu(summed[2]) * summed[3]).astype(jnp.bfloat16)
    expert_rows = local_product(routed_hidden, down_matrix).astype(jnp.bfloat16)
    shared_out = local_product(shared_hidden, shared_down)
    own_expert = lax.axis_index("ep")
    column = lax.dynamic_slice_in_dim(table_all, own_expert, 1, 1)
    routed = lax.psum_scatter(
        (column * expert_rows.astype(jnp.float32)).astype(jnp.bfloat16),
        "ep",
        scatter_dimension=0,
        tiled=True,
    ).astype(jnp.float32)
    mixture = routed + shared_out
    square_sum = lax.psum(jnp.sum(mixture * mixture, axis=-1, keepdims=True), "tp")
    scale = lax.rsqrt(square_sum / full_width + epsilon)
    return (mixture * scale * out_gain).astype(jnp.bfloat16)


def solution(mesh):
    chips = mesh.shape["ep"] // 2
    if mesh.shape["tp"] == 2 and mesh.shape["ep"] == 8:
        body = functools.partial(fused, chips)
    else:
        body = per_device
    return jax.shard_map(
        body,
        mesh=mesh,
        in_specs=(
            P(("grp", "ep"), "tp"),
            P(("grp", "ep"), None),
            P(("grp", "ep"), None),
            P(),
            P("ep", "tp", None),
            P("ep", "tp", None),
            P("ep", None, "tp"),
            P("tp", None),
            P("tp", None),
            P(None, "tp"),
            P("tp"),
        ),
        out_specs=P(("grp", "ep"), "tp"),
        check_vma=False,
    )
```

```python
import functools

import jax
import jax.numpy as jnp
from jax import lax
from jax.experimental import pallas as pl
from jax.experimental.pallas import tpu as pltpu
from jax.sharding import PartitionSpec as P

epsilon = 1e-06
MESH = pl.DeviceIdType.MESH


NEAR, MIDDLE, FAR, SPARE, MIXTURE = range(5)
STEPS = (
    "own",
    (NEAR, 0),
    (MIDDLE, 0),
    (FAR, 0),
    (FAR, 1),
    (MIDDLE, 1),
    (NEAR, 1),
    "other",
)


def pick(index, table):
    value = jnp.int32(table[0])
    for position in range(1, len(table)):
        if table[position] != table[0]:
            value = jnp.where(index == position, jnp.int32(table[position]), value)
    return value


def exclusive_or(a, b, size):
    total, unit = jnp.int32(0), 1
    while unit < size:
        total = total + unit * lax.rem(lax.div(a, unit) + lax.div(b, unit), 2)
        unit *= 2
    return total


def fused_kernel(
    chips,
    tokens_hbm,
    routes_hbm,
    weights_hbm,
    norm_gain_hbm,
    gate_hbm,
    up_hbm,
    down_hbm,
    shared_gate_hbm,
    shared_up_hbm,
    shared_down_hbm,
    out_gain_hbm,
    out_ref,
    routes_ref,
    weights_ref,
    norm_gain_ref,
    out_gain_ref,
    gate,
    up,
    down,
    held,
    source,
    part_out,
    part_in,
    part_own,
    hidden,
    product,
    sums,
    pair_out,
    pair_in,
    far_out,
    far_in,
    square_out,
    square_in,
    info,
    load_sem,
    info_send,
    info_recv,
    pair_info_recv,
    square_send,
    square_recv,
    gather_send,
    gather_recv,
    pair_gather_recv,
    part_send,
    part_recv,
    hidden_send,
    hidden_recv,
    pair_send,
    pair_recv,
    far_send,
    far_recv,
):
    rows, width = product.shape
    mixture = sums.at[MIXTURE]
    experts = 2 * chips
    units = gate.shape[2]
    half = units // 2
    count = len(STEPS)
    slots = [step[0] if isinstance(step, tuple) else NEAR for step in STEPS]
    lanes = [
        [side if step == "own" else 1 - side if step == "other" else step[1] if isinstance(step, tuple) else side for step in STEPS]
        for side in range(2)
    ]
    quarter = half // 2
    other_at, shared_at = count - 1, count

    ep = lax.axis_index("ep")
    tp = lax.axis_index("tp")
    chip, core = lax.div(ep, 2), lax.rem(ep, 2)
    other_core = 1 - core
    partner = {"ep": chip * 2 + other_core}
    across = {"tp": 1 - tp}

    away = pl.ds(pl.multiple_of((1 - tp) * half, half), half)
    near = pl.ds(pl.multiple_of(tp * half, half), half)
    features = pl.ds(pl.multiple_of(tp * width, width), width)
    groups = [
        [(tokens_hbm, held.at[ep])],
        [(norm_gain_hbm.at[:, features], norm_gain_ref)],
        [(gate_hbm.at[0, :, away], gate.at[0, :, away])],
        [(up_hbm.at[0, :, away], up.at[0, :, away])],
        [
            (gate_hbm.at[0, :, near], gate.at[0, :, near]),
            (up_hbm.at[0, :, near], up.at[0, :, near]),
        ],
        [(routes_hbm, routes_ref), (weights_hbm, weights_ref)],
        [(shared_gate_hbm, gate.at[1]), (shared_up_hbm, up.at[1])],
        [(down_hbm.at[0], down.at[0]), (shared_down_hbm, down.at[1])],
        [(out_gain_hbm, out_gain_ref)],
    ]
    wholes = [held.at[ep], norm_gain_ref, gate.at[0, :, away], up.at[0, :, away]]
    wholes += [gate.at[0], info.at[0, :8], gate, down, out_gain_ref]
    names = ["tokens", "norm_gain", "gate_away", "up_away", "near", "table"]
    names += ["shared_in", "down", "out_gain"]

    loads = {
        name: pltpu.make_async_copy(whole, whole, load_sem.at[i])
        for i, (name, whole) in enumerate(zip(names, wholes))
    }
    for i, group in enumerate(groups):
        for load_from, load_to in group:
            pltpu.make_async_copy(load_from, load_to, load_sem.at[i]).start()

    barrier = pltpu.get_barrier_semaphore()
    def greet(device):
        pl.semaphore_signal(barrier, inc=1, device_id=device, device_id_type=MESH)

    greet(across)
    greet(partner)

    @pl.when(chip > 0)
    def _():
        greet({"ep": (chip - 1) * 2 + core})

    @pl.when(chip < chips - 1)
    def _():
        greet({"ep": (chip + 1) * 2 + core})

    def remote(source, target, send, recv, device):
        return pltpu.make_async_remote_copy(
            src_ref=source,
            dst_ref=target,
            send_sem=send,
            recv_sem=recv,
            device_id=device,
            device_id_type=MESH,
        )

    def square_copy(which):
        return remote(
            square_out.at[which],
            square_in.at[which],
            square_send.at[which],
            square_recv.at[which],
            across,
        )

    def ways(way):
        return ({"ep": (chip - 1) * 2 + core}, {"ep": (chip + 1) * 2 + core}, partner)[way]

    def tokens_copy(origin, way):
        slot = held.at[origin * 2 + core]
        recv = (pair_gather_recv if way == 2 else gather_recv).at[origin]
        return remote(slot, slot, gather_send.at[way // 2], recv, ways(way))

    def info_copy(origin, way):
        slot = info.at[origin * 2 + core]
        recv = (pair_info_recv if way == 2 else info_recv).at[origin]
        return remote(slot, slot, info_send.at[way // 2], recv, ways(way))

    def pass_on(origin, way):
        tokens_copy(origin, way).start()
        info_copy(origin, way).start()

    def pair_info_arrival(origin):
        slot = info.at[origin * 2 + other_core]
        return remote(slot, slot, info_send.at[1], pair_info_recv.at[origin], partner)

    def pair_gather_arrival(origin):
        slot = held.at[origin * 2 + other_core]
        return remote(slot, slot, gather_send.at[1], pair_gather_recv.at[origin], partner)

    def part_copy(k, which):
        place = lax.rem(k, 3)
        return remote(
            part_out.at[k, which],
            part_in.at[k, which],
            part_send.at[0],
            part_recv.at[place],
            across,
        )

    def part_arrival(k):
        place = lax.rem(k, 3)
        return remote(
            part_out.at[k], part_in.at[k], part_send.at[0], part_recv.at[place], across
        )

    def shared_part_copy(piece):
        return remote(
            part_out.at[shared_at, piece],
            part_in.at[shared_at, piece],
            part_send.at[0],
            part_recv.at[3 + piece],
            across,
        )

    def hidden_copy(k, side):
        slot = hidden.at[k, side]
        return remote(slot, slot, hidden_send.at[0], hidden_recv.at[lax.rem(k, 4)], across)

    def shared_copy(piece, side):
        slot = hidden.at[shared_at, side, :, piece * quarter : (piece + 1) * quarter]
        return remote(slot, slot, hidden_send.at[0], hidden_recv.at[4 + piece], across)

    def part_of(piece):
        return pl.ds(piece * (width // 2), width // 2)

    def pair_copy(origin, piece):
        return remote(
            pair_out.at[origin, :, part_of(piece)],
            pair_in.at[origin, :, part_of(piece)],
            pair_send.at[0],
            pair_recv.at[origin, piece],
            partner,
        )

    beside, opposite, beyond = (exclusive_or(chip, mask, chips) for mask in (1, 2, 3))
    outer = (chip == 0) | (chip == chips - 1)
    inner = jnp.logical_not(outer)

    def origin_of(slot):
        middle, far = jnp.where(outer, opposite, beyond), jnp.where(outer, beyond, opposite)
        return jnp.where(slot == NEAR, beside, jnp.where(slot == MIDDLE, middle, far))

    def far_copy(slot, piece):
        direct = outer | (slot == NEAR)
        place = jnp.where(direct, slot, FAR + 1)
        target = jnp.where(direct, beside, origin_of(slot))
        return remote(
            far_out.at[slot, :, part_of(piece)],
            far_in.at[place, :, part_of(piece)],
            far_send.at[0],
            far_recv.at[place, piece],
            {"ep": target * 2 + core},
        )

    def far_arrival(place, piece):
        return remote(
            far_out.at[0, :, part_of(piece)],
            far_in.at[place, :, part_of(piece)],
            far_send.at[0],
            far_recv.at[place, piece],
            {"ep": beside * 2 + core},
        )

    def pack(column):
        return jnp.transpose(jnp.broadcast_to(column, (rows, 128)))[:8]

    def unpack(row):
        return jnp.transpose(jnp.broadcast_to(row[:1], (128, rows)))

    def across_lanes(column, lanes):
        return jnp.concatenate([column] * (lanes // 128), axis=1)

    loads["tokens"].wait()
    token_float = held[ep].astype(jnp.float32)
    own_square = jnp.sum(token_float * token_float, axis=-1, keepdims=True)
    square_out[0] = pack(own_square)
    pl.semaphore_wait(barrier, jnp.where((chip == 0) | (chip == chips - 1), 3, 4))

    def send_outward(copy):
        @pl.when((core == 0) & (chip > 0))
        def _():
            copy(chip, 0).start()

        @pl.when((core == 0) & (chip < chips - 1))
        def _():
            copy(chip, 1).start()

        copy(chip, 2).start()

    send_outward(tokens_copy)
    square_copy(0).start()
    loads["norm_gain"].wait()

    def share_info():
        loads["table"].wait()
        expert_ids = lax.broadcasted_iota(jnp.int32, (experts, rows), 0)
        table = jnp.zeros((experts, rows), jnp.float32)
        for choice in range(routes_ref.shape[0]):
            match = expert_ids == routes_ref[choice : choice + 1, :]
            table = table + jnp.where(match, weights_ref[choice : choice + 1, :], 0.0)
        info[ep, :experts] = table
        square_copy(0).wait_recv()
        square = square_out[0] + square_in[0]
        info[ep, experts:] = lax.rsqrt(square / (2 * width) + epsilon)
        send_outward(info_copy)

    def take(origin):
        tokens_copy(origin, 0).wait_recv()
        info_copy(origin, 0).wait_recv()
        pass_on(origin, 2)

    def toward_outer(origin):
        @pl.when(chip == 1)
        def _():
            pass_on(origin, 0)

        @pl.when(chip == chips - 2)
        def _():
            pass_on(origin, 1)

    def toward_inner(origin):
        @pl.when(chip < chips // 2)
        def _():
            pass_on(origin, 1)

        @pl.when(chip >= chips // 2)
        def _():
            pass_on(origin, 0)

    def relay(distance):
        @pl.when(chip >= distance)
        def _():
            take(chip - distance)

            @pl.when(chip < chips - 1)
            def _():
                pass_on(chip - distance, 1)

        @pl.when(chip + distance < chips)
        def _():
            take(chip + distance)

            @pl.when(chip > 0)
            def _():
                pass_on(chip + distance, 0)

    def second_lane_before(i):
        @pl.when((i == 4) & inner)
        def _():
            take(beyond)
            toward_outer(beyond)
            toward_outer(chip)

        @pl.when((i >= 4) & (i < 7) & outer)
        def _():
            take(origin_of(pick(i, slots)))

    def second_lane_after(i):
        @pl.when((i == 2) & inner)
        def _():
            take(beside)
            toward_inner(beside)
            toward_inner(chip)

        @pl.when((i == 3) & inner)
        def _():
            take(opposite)
            toward_outer(opposite)

    def locate(k):
        away_from = origin_of(pick(k, slots))
        origin = jnp.where((k == 0) | (k == other_at), chip, away_from)
        lane = jnp.where(core == 0, pick(k, lanes[0]), pick(k, lanes[1]))
        return origin, lane

    def block_of(k):
        origin, lane = locate(k)
        return origin * 2 + lane

    def scaled(block):
        source[...] = (held[block].astype(jnp.float32) * norm_gain_ref[...]).astype(jnp.bfloat16)

    def product_of(matrix, columns):
        return jnp.dot(
            source[...], matrix[columns], preferred_element_type=jnp.float32
        ).astype(jnp.bfloat16)

    def first_stage(k):
        origin, lane = locate(k)
        pl.when((k == 2) & (core == 0) & outer)(functools.partial(relay, 2))
        pl.when((k == 3) & (core == 0))(functools.partial(relay, 3))

        @pl.when(lane != core)
        def _():
            pair_gather_arrival(origin).wait_recv()

        scaled(block_of(k))
        pl.when(k == 0)(loads["gate_away"].wait)
        part_out[k, 0] = product_of(gate.at[0], (slice(None), away))
        part_copy(k, 0).start()

    def finish_first_stage(k):
        pl.when(k == 0)(loads["up_away"].wait)
        part_out[k, 1] = product_of(up.at[0], (slice(None), away))
        part_copy(k, 1).start()
        pl.when(k == 0)(loads["near"].wait)
        for which, matrix in enumerate((gate, up)):
            part_own[k, which] = product_of(matrix.at[0], (slice(None), near))

    def piece_of(side, piece):
        return pl.ds(pl.multiple_of(side * half + piece * quarter, quarter), quarter)

    def shared_first(piece):
        if piece == 0:
            loads["shared_in"].wait()
        else:
            scaled(ep)
        for side, target in ((1 - tp, part_out), (tp, part_own)):
            columns = (slice(None), piece_of(side, piece))
            for which, matrix in enumerate((gate, up)):
                place = slice(which * quarter, (which + 1) * quarter)
                target[shared_at, piece, :, place] = product_of(matrix.at[1], columns)
            if target is part_out:
                shared_part_copy(piece).start()

    def shared_second(piece):
        scale = across_lanes(unpack(info[ep, experts : experts + 1]), half)
        shared_part_copy(piece).wait_recv()
        total = part_own[shared_at, piece].astype(jnp.float32)
        total = (total + part_in[shared_at, piece].astype(jnp.float32)) * scale
        product_out = jax.nn.silu(total[:, :quarter]) * total[:, quarter:]
        place = slice(piece * quarter, (piece + 1) * quarter)
        hidden[shared_at, tp, :, place] = product_out.astype(jnp.bfloat16)
        shared_copy(piece, tp).start()

    def shared_product(piece, side, columns):
        place = slice(piece * quarter, (piece + 1) * quarter)
        return jnp.dot(
            hidden[shared_at, side, :, place],
            down[1, piece_of(side, piece), columns],
            preferred_element_type=jnp.float32,
        )

    def shared_third():
        def own_step(columns):
            mixture[:, columns] += shared_product(0, tp, columns)

        def other_step(columns):
            mixture[:, columns] += shared_product(0, 1 - tp, columns)

        tiles(own_step)
        shared_copy(0, 1 - tp).wait_recv()
        tiles(other_step)

    def second_stage(k):
        block = block_of(k)

        origin, lane = locate(k)

        @pl.when(lane != core)
        def _():
            pair_info_arrival(origin).wait_recv()

        scale = across_lanes(unpack(info[block, experts : experts + 1]), half)
        part_arrival(k).wait_recv()
        gate_sum = part_own[k, 0].astype(jnp.float32) + part_in[k, 0].astype(jnp.float32)
        up_sum = part_own[k, 1].astype(jnp.float32) + part_in[k, 1].astype(jnp.float32)
        gate_sum, up_sum = gate_sum * scale, up_sum * scale
        hidden[k, tp] = (jax.nn.silu(gate_sum) * up_sum).astype(jnp.bfloat16)
        hidden_copy(k, tp).start()

    def down_product(k, side, columns):
        rows_of = pl.ds(pl.multiple_of(side * half, half), half)
        return jnp.dot(
            hidden[k, side], down[0, rows_of, columns], preferred_element_type=jnp.float32
        )

    tile = width // 4

    def tiles(step, first=0, last=4):
        def tile_step(i, carry):
            step(pl.ds(pl.multiple_of(i * tile, tile), tile))
            return carry

        lax.fori_loop(first, last, tile_step, 0)

    def third_stage(k):
        origin, lane = locate(k)
        pl.when(k == 0)(loads["down"].wait)

        def own_step(columns):
            product[:, columns] = down_product(k, tp, columns)

        keeper = lane == core
        kept = jnp.where(keeper, jnp.where(k == 0, MIXTURE, pick(k, slots)), SPARE)
        sent = jnp.where(keeper, chips, origin)

        def other_step(columns):
            total = product[:, columns] + down_product(k, 1 - tp, columns)
            weighted = total.astype(jnp.bfloat16).astype(jnp.float32) * scale
            sums[kept, :, columns] = weighted
            pair_out[sent, :, columns] = weighted.astype(jnp.bfloat16)

        tiles(own_step, 0, 4)
        scale = across_lanes(unpack(info[block_of(k), pl.ds(ep, 1)]), tile)
        hidden_copy(k, 1 - tp).wait_recv()
        for piece in range(2):
            tiles(other_step, 2 * piece, 2 * piece + 2)

            @pl.when(lane != core)
            def _(piece=piece):
                pair_copy(origin, piece).start()

    def fourth_stage(k):
        origin, lane = locate(k)

        @pl.when((k != 0) & (lane == core))
        def _():
            slot = pick(k, slots)
            direct = outer | (slot == NEAR)
            for piece in range(2):
                columns = part_of(piece)
                pair_copy(origin, piece).wait_recv()
                total = sums[slot, :, columns] + pair_in[origin, :, columns].astype(jnp.float32)
                sums[slot, :, columns] = total
                far_out[slot, :, columns] = total.astype(jnp.bfloat16)

                @pl.when(direct & (outer | (k != 1)))
                def _(piece=piece):
                    far_copy(slot, piece).start()

    def fifth_stage(k):
        slot = pick(k, slots)
        for piece in range(2):
            columns = part_of(piece)
            far_arrival(slot, piece).wait_recv()
            total = sums[slot, :, columns] + far_in[slot, :, columns].astype(jnp.float32)
            far_out[slot, :, columns] = total.astype(jnp.bfloat16)
            far_copy(slot, piece).start()

    def body(i, carry):
        early, late = i <= 3, (i >= 4) & (i <= count)
        pl.when(core == 1)(functools.partial(second_lane_before, i))

        @pl.when(i == 4)
        def _():
            fourth_stage(1)

        @pl.when((i == 6) & (core == 0) & inner)
        def _():
            far_copy(NEAR, 0).start()
            far_copy(NEAR, 1).start()

        @pl.when(i == 1)
        def _():
            pl.when(core == 0)(functools.partial(relay, 1))
            second_stage(0)
            pl.when((core == 1) & outer)(functools.partial(toward_inner, chip))

        @pl.when(i < count)
        def _():
            first_stage(i)

        @pl.when(i == count)
        def _():
            shared_first(1)

        @pl.when(early)
        def _():
            finish_first_stage(i)

        pl.when(core == 1)(functools.partial(second_lane_after, i))

        @pl.when(i == 0)
        def _():
            share_info()
            shared_first(0)

        @pl.when(i == 1)
        def _():
            shared_second(0)

        @pl.when(late)
        def _():
            third_stage(i - 2)

        pl.when((i == 2) & (core == 0) & inner)(functools.partial(relay, 2))

        @pl.when((i >= 2) & (i <= count))
        def _():
            second_stage(i - 1)

        @pl.when(late)
        def _():
            fourth_stage(i - 2)

        @pl.when(late & (i < count))
        def _():
            finish_first_stage(i)

        @pl.when(inner & jnp.where(core == 0, (i == 5) | (i == 6), (i == 7) | (i == 8)))
        def _():
            fifth_stage(i - 3)

        @pl.when(i == count + 1)
        def _():
            shared_second(1)

        @pl.when((i == 2) | (i == 3) | (i == count + 1))
        def _():
            third_stage(i - 2)

        pl.when(i == 3)(shared_third)
        return carry

    lax.fori_loop(0, count + 2, body, 0)

    def shared_own(columns):
        mixture[:, columns] += shared_product(1, tp, columns)

    tiles(shared_own)
    for piece in range(2):
        pair_copy(chip, piece).wait_recv()
        mixture[:, part_of(piece)] += pair_in[chip, :, part_of(piece)].astype(jnp.float32)
    for place in (FAR + 1, NEAR):
        for piece in range(2):
            columns = part_of(piece)
            far_arrival(place, piece).wait_recv()
            mixture[:, columns] += far_in[place, :, columns].astype(jnp.float32)
    shared_copy(1, 1 - tp).wait_recv()
    own_total = jnp.zeros((rows, 1), jnp.float32)
    for start in range(0, width, tile):
        columns = slice(start, start + tile)
        mixed = mixture[:, columns] + shared_product(1, 1 - tp, columns)
        mixture[:, columns] = mixed
        own_total = own_total + jnp.sum(mixed * mixed, axis=-1, keepdims=True)
    square_out[1] = pack(own_total)
    square_copy(1).start()
    loads["out_gain"].wait()
    mixture[...] *= out_gain_ref[...]
    square_copy(0).wait_send()
    square_copy(1).wait_send()

    def sent(whole, sem):
        pltpu.make_async_copy(whole, whole, sem.at[0]).wait()

    for whole, sem in ((held, gather_send), (info, info_send)):

        @pl.when(outer)
        def _(whole=whole, sem=sem):
            pltpu.make_async_copy(whole.at[0], whole.at[0], sem.at[0]).wait()

        @pl.when(inner)
        def _(whole=whole, sem=sem):
            several = whole.at[: chips + 1]
            pltpu.make_async_copy(several, several, sem.at[0]).wait()

        pltpu.make_async_copy(whole.at[:chips], whole.at[:chips], sem.at[1]).wait()

    sent(part_out, part_send)
    sent(part_out.at[:, 0], hidden_send)
    sent(pair_in, pair_send)
    sent(far_out, far_send)
    square_copy(1).wait_recv()
    scale = lax.rsqrt((own_total + unpack(square_in[1])) / (2 * width) + epsilon)
    out_ref[...] = (mixture[...] * across_lanes(scale, width)).astype(jnp.bfloat16)


def fused(
    chips,
    tokens,
    routes,
    route_weights,
    norm_gain,
    expert_gate,
    expert_up,
    expert_down,
    shared_gate,
    shared_up,
    shared_down,
    out_gain,
):
    rows, width = tokens.shape
    units = shared_gate.shape[1]
    half = units // 2
    count = 2 * chips + 1
    choices = routes.shape[1]
    vmem = pl.BlockSpec(memory_space=pltpu.VMEM)
    hbm = pl.BlockSpec(memory_space=pl.ANY)
    bf16, f32 = jnp.bfloat16, jnp.float32
    dma = pltpu.SemaphoreType.DMA
    return pl.pallas_call(
        functools.partial(fused_kernel, chips),
        out_shape=pltpu.VMEM((rows, width), bf16),
        in_specs=[hbm] * 11,
        out_specs=vmem,
        scratch_shapes=[
            pltpu.VMEM((choices, rows), jnp.int32),
            pltpu.VMEM((choices, rows), f32),
            pltpu.VMEM((1, width), f32),
            pltpu.VMEM((1, width), f32),
            pltpu.VMEM((2, width, units), bf16),
            pltpu.VMEM((2, width, units), bf16),
            pltpu.VMEM((2, units, width), bf16),
            pltpu.VMEM((2 * chips, rows, width), bf16),
            pltpu.VMEM((rows, width), bf16),
            pltpu.VMEM((count, 2, rows, half), bf16),
            pltpu.VMEM((count, 2, rows, half), bf16),
            pltpu.VMEM((count, 2, rows, half), bf16),
            pltpu.VMEM((count, 2, rows, half), bf16),
            pltpu.VMEM((rows, width), f32),
            pltpu.VMEM((5, rows, width), f32),
            pltpu.VMEM((chips + 1, rows, width), bf16),
            pltpu.VMEM((chips, rows, width), bf16),
            pltpu.VMEM((3, rows, width), bf16),
            pltpu.VMEM((4, rows, width), bf16),
            pltpu.VMEM((2, 8, rows), f32),
            pltpu.VMEM((2, 8, rows), f32),
            pltpu.VMEM((2 * chips, 2 * chips + 8, rows), f32),
            dma((9,)),
            dma((2,)),
            dma((chips,)),
            dma((chips,)),
            dma((2,)),
            dma((2,)),
            dma((2,)),
            dma((chips,)),
            dma((chips,)),
            dma((1,)),
            dma((5,)),
            dma((1,)),
            dma((6,)),
            dma((1,)),
            dma((chips, 2)),
            dma((1,)),
            dma((4, 2)),
        ],
        compiler_params=pltpu.CompilerParams(
            collective_id=0, has_side_effects=True, vmem_limit_bytes=60 * 1024 * 1024
        ),
    )(
        tokens,
        routes.T,
        route_weights.T,
        norm_gain.reshape(1, -1),
        expert_gate,
        expert_up,
        expert_down,
        shared_gate,
        shared_up,
        shared_down,
        out_gain.reshape(1, -1),
    )


def local_product(source, matrix):
    return jnp.dot(source, matrix, preferred_element_type=jnp.float32)


def per_device(
    tokens,
    routes,
    route_weights,
    norm_gain,
    expert_gate,
    expert_up,
    expert_down,
    shared_gate,
    shared_up,
    shared_down,
    out_gain,
):
    block_width = tokens.shape[1]
    full_width = block_width * lax.axis_size("tp")
    width_index = lax.axis_index("tp")
    full_rows = lax.all_gather(tokens, "tp", axis=1, tiled=True)
    full_float = full_rows.astype(jnp.float32)
    normed_full = (
        full_float
        * lax.rsqrt(jnp.mean(full_float * full_float, axis=-1, keepdims=True) + epsilon)
        * norm_gain
    ).astype(jnp.bfloat16)
    normed_block = lax.dynamic_slice_in_dim(normed_full, width_index * block_width, block_width, 1)
    gate_matrix = expert_gate[0]
    up_matrix = expert_up[0]
    down_matrix = expert_down[0]
    experts = lax.axis_size("ep")
    choose = (routes[:, :, None] == jnp.arange(experts, dtype=jnp.int32)[None, None, :]).astype(
        jnp.float32
    )
    weight_table = jnp.sum(route_weights[:, :, None] * choose, axis=1)
    expert_input = lax.all_gather(normed_block, "ep", axis=0, tiled=True)
    table_all = lax.all_gather(weight_table, "ep", axis=0, tiled=True)
    summed = (
        lax.psum(local_product(expert_input, gate_matrix).astype(jnp.bfloat16), "tp").astype(
            jnp.float32
        ),
        lax.psum(local_product(expert_input, up_matrix).astype(jnp.bfloat16), "tp").astype(
            jnp.float32
        ),
        lax.psum(local_product(normed_block, shared_gate).astype(jnp.bfloat16), "tp").astype(
            jnp.float32
        ),
        lax.psum(local_product(normed_block, shared_up).astype(jnp.bfloat16), "tp").astype(
            jnp.float32
        ),
    )
    routed_hidden = (jax.nn.silu(summed[0]) * summed[1]).astype(jnp.bfloat16)
    shared_hidden = (jax.nn.silu(summed[2]) * summed[3]).astype(jnp.bfloat16)
    expert_rows = local_product(routed_hidden, down_matrix).astype(jnp.bfloat16)
    shared_out = local_product(shared_hidden, shared_down)
    own_expert = lax.axis_index("ep")
    column = lax.dynamic_slice_in_dim(table_all, own_expert, 1, 1)
    routed = lax.psum_scatter(
        (column * expert_rows.astype(jnp.float32)).astype(jnp.bfloat16),
        "ep",
        scatter_dimension=0,
        tiled=True,
    ).astype(jnp.float32)
    mixture = routed + shared_out
    square_sum = lax.psum(jnp.sum(mixture * mixture, axis=-1, keepdims=True), "tp")
    scale = lax.rsqrt(square_sum / full_width + epsilon)
    return (mixture * scale * out_gain).astype(jnp.bfloat16)


def solution(mesh):
    chips = mesh.shape["ep"] // 2
    if mesh.shape["tp"] == 2 and mesh.shape["ep"] == 8:
        body = functools.partial(fused, chips)
    else:
        body = per_device
    return jax.shard_map(
        body,
        mesh=mesh,
        in_specs=(
            P(("grp", "ep"), "tp"),
            P(("grp", "ep"), None),
            P(("grp", "ep"), None),
            P(),
            P("ep", "tp", None),
            P("ep", "tp", None),
            P("ep", None, "tp"),
            P("tp", None),
            P("tp", None),
            P(None, "tp"),
            P("tp"),
        ),
        out_specs=P(("grp", "ep"), "tp"),
        check_vma=False,
    )
```

```python
import functools

import jax
import jax.numpy as jnp
from jax import lax
from jax.experimental import pallas as pl
from jax.experimental.pallas import tpu as pltpu
from jax.sharding import PartitionSpec as P

epsilon = 1e-06
MESH = pl.DeviceIdType.MESH


NEAR, MIDDLE, FAR, SPARE, MIXTURE = range(5)
STEPS = (
    "own",
    (NEAR, 0),
    (MIDDLE, 0),
    (FAR, 0),
    (FAR, 1),
    (MIDDLE, 1),
    (NEAR, 1),
    "other",
)


def pick(index, table):
    value = jnp.int32(table[0])
    for position in range(1, len(table)):
        if table[position] != table[0]:
            value = jnp.where(index == position, jnp.int32(table[position]), value)
    return value


def exclusive_or(a, b, size):
    total, unit = jnp.int32(0), 1
    while unit < size:
        total = total + unit * lax.rem(lax.div(a, unit) + lax.div(b, unit), 2)
        unit *= 2
    return total


def fused_kernel(
    chips,
    tokens_hbm,
    routes_hbm,
    weights_hbm,
    norm_gain_hbm,
    gate_hbm,
    up_hbm,
    down_hbm,
    shared_gate_hbm,
    shared_up_hbm,
    shared_down_hbm,
    out_gain_hbm,
    out_ref,
    routes_ref,
    weights_ref,
    norm_gain_ref,
    out_gain_ref,
    gate,
    up,
    down,
    held,
    source,
    part_out,
    part_in,
    part_own,
    hidden,
    product,
    sums,
    pair_out,
    pair_in,
    far_out,
    far_in,
    square_out,
    square_in,
    info,
    load_sem,
    info_send,
    info_recv,
    pair_info_recv,
    square_send,
    square_recv,
    gather_send,
    gather_recv,
    pair_gather_recv,
    part_send,
    part_recv,
    hidden_send,
    hidden_recv,
    pair_send,
    pair_recv,
    far_send,
    far_recv,
):
    rows, width = product.shape
    mixture = sums.at[MIXTURE]
    experts = 2 * chips
    units = gate.shape[2]
    half = units // 2
    count = len(STEPS)
    slots = [step[0] if isinstance(step, tuple) else NEAR for step in STEPS]
    lanes = [
        [side if step == "own" else 1 - side if step == "other" else step[1] if isinstance(step, tuple) else side for step in STEPS]
        for side in range(2)
    ]
    quarter = half // 2
    other_at, shared_at = count - 1, count

    ep = lax.axis_index("ep")
    tp = lax.axis_index("tp")
    chip, core = lax.div(ep, 2), lax.rem(ep, 2)
    other_core = 1 - core
    partner = {"ep": chip * 2 + other_core}
    across = {"tp": 1 - tp}

    away = pl.ds(pl.multiple_of((1 - tp) * half, half), half)
    near = pl.ds(pl.multiple_of(tp * half, half), half)
    features = pl.ds(pl.multiple_of(tp * width, width), width)
    groups = [
        [(tokens_hbm, held.at[ep])],
        [(norm_gain_hbm.at[:, features], norm_gain_ref)],
        [(gate_hbm.at[0, :, away], gate.at[0, :, away])],
        [(up_hbm.at[0, :, away], up.at[0, :, away])],
        [
            (gate_hbm.at[0, :, near], gate.at[0, :, near]),
            (up_hbm.at[0, :, near], up.at[0, :, near]),
        ],
        [(routes_hbm, routes_ref), (weights_hbm, weights_ref)],
        [(shared_gate_hbm, gate.at[1]), (shared_up_hbm, up.at[1])],
        [(down_hbm.at[0], down.at[0]), (shared_down_hbm, down.at[1])],
        [(out_gain_hbm, out_gain_ref)],
    ]
    wholes = [held.at[ep], norm_gain_ref, gate.at[0, :, away], up.at[0, :, away]]
    wholes += [gate.at[0], info.at[0, :8], gate, down, out_gain_ref]
    names = ["tokens", "norm_gain", "gate_away", "up_away", "near", "table"]
    names += ["shared_in", "down", "out_gain"]

    loads = {
        name: pltpu.make_async_copy(whole, whole, load_sem.at[i])
        for i, (name, whole) in enumerate(zip(names, wholes))
    }
    for i, group in enumerate(groups):
        for load_from, load_to in group:
            pltpu.make_async_copy(load_from, load_to, load_sem.at[i]).start()

    barrier = pltpu.get_barrier_semaphore()
    def greet(device):
        pl.semaphore_signal(barrier, inc=1, device_id=device, device_id_type=MESH)

    greet(across)
    greet(partner)

    @pl.when(chip > 0)
    def _():
        greet({"ep": (chip - 1) * 2 + core})

    @pl.when(chip < chips - 1)
    def _():
        greet({"ep": (chip + 1) * 2 + core})

    def remote(source, target, send, recv, device):
        return pltpu.make_async_remote_copy(
            src_ref=source,
            dst_ref=target,
            send_sem=send,
            recv_sem=recv,
            device_id=device,
            device_id_type=MESH,
        )

    def square_copy(which):
        return remote(
            square_out.at[which],
            square_in.at[which],
            square_send.at[which],
            square_recv.at[which],
            across,
        )

    def ways(way):
        return ({"ep": (chip - 1) * 2 + core}, {"ep": (chip + 1) * 2 + core}, partner)[way]

    def tokens_copy(origin, way):
        slot = held.at[origin * 2 + core]
        recv = (pair_gather_recv if way == 2 else gather_recv).at[origin]
        return remote(slot, slot, gather_send.at[way // 2], recv, ways(way))

    def info_copy(origin, way):
        slot = info.at[origin * 2 + core]
        recv = (pair_info_recv if way == 2 else info_recv).at[origin]
        return remote(slot, slot, info_send.at[way // 2], recv, ways(way))

    def pass_on(origin, way):
        tokens_copy(origin, way).start()
        info_copy(origin, way).start()

    def pair_info_arrival(origin):
        slot = info.at[origin * 2 + other_core]
        return remote(slot, slot, info_send.at[1], pair_info_recv.at[origin], partner)

    def pair_gather_arrival(origin):
        slot = held.at[origin * 2 + other_core]
        return remote(slot, slot, gather_send.at[1], pair_gather_recv.at[origin], partner)

    def part_copy(k, which):
        place = lax.rem(k, 3)
        return remote(
            part_out.at[k, which],
            part_in.at[k, which],
            part_send.at[0],
            part_recv.at[place],
            across,
        )

    def part_arrival(k):
        place = lax.rem(k, 3)
        return remote(
            part_out.at[k], part_in.at[k], part_send.at[0], part_recv.at[place], across
        )

    def shared_part_copy(piece):
        return remote(
            part_out.at[shared_at, piece],
            part_in.at[shared_at, piece],
            part_send.at[0],
            part_recv.at[3 + piece],
            across,
        )

    def hidden_copy(k, side):
        slot = hidden.at[k, side]
        return remote(slot, slot, hidden_send.at[0], hidden_recv.at[lax.rem(k, 4)], across)

    def shared_copy(piece, side):
        slot = hidden.at[shared_at, side, :, piece * quarter : (piece + 1) * quarter]
        return remote(slot, slot, hidden_send.at[0], hidden_recv.at[4 + piece], across)

    def part_of(piece):
        return pl.ds(piece * (width // 2), width // 2)

    def pair_copy(origin, piece):
        return remote(
            pair_out.at[origin, :, part_of(piece)],
            pair_in.at[origin, :, part_of(piece)],
            pair_send.at[0],
            pair_recv.at[origin, piece],
            partner,
        )

    beside, opposite, beyond = (exclusive_or(chip, mask, chips) for mask in (1, 2, 3))
    outer = (chip == 0) | (chip == chips - 1)
    inner = jnp.logical_not(outer)

    def origin_of(slot):
        middle, far = jnp.where(outer, opposite, beyond), jnp.where(outer, beyond, opposite)
        return jnp.where(slot == NEAR, beside, jnp.where(slot == MIDDLE, middle, far))

    def far_copy(slot, piece):
        direct = outer | (slot == NEAR)
        place = jnp.where(direct, slot, FAR + 1)
        target = jnp.where(direct, beside, origin_of(slot))
        return remote(
            far_out.at[slot, :, part_of(piece)],
            far_in.at[place, :, part_of(piece)],
            far_send.at[0],
            far_recv.at[place, piece],
            {"ep": target * 2 + core},
        )

    def far_arrival(place, piece):
        return remote(
            far_out.at[0, :, part_of(piece)],
            far_in.at[place, :, part_of(piece)],
            far_send.at[0],
            far_recv.at[place, piece],
            {"ep": beside * 2 + core},
        )

    def row_squares(values):
        total = jnp.zeros((rows, 128), jnp.float32)
        for start in range(0, values.shape[1], 128):
            chunk = values[:, start : start + 128]
            total = total + chunk * chunk
        return total

    def pack(partial):
        row = jnp.sum(jnp.transpose(partial), axis=0, keepdims=True)
        return jnp.broadcast_to(row, (8, rows))

    def unpack(row):
        return jnp.transpose(jnp.broadcast_to(row[:1], (128, rows)))

    def across_lanes(column, lanes):
        return jnp.concatenate([column] * (lanes // 128), axis=1)

    loads["tokens"].wait()
    square_out[0] = pack(row_squares(held[ep].astype(jnp.float32)))
    pl.semaphore_wait(barrier, jnp.where((chip == 0) | (chip == chips - 1), 3, 4))

    def send_outward(copy):
        @pl.when((core == 0) & (chip > 0))
        def _():
            copy(chip, 0).start()

        @pl.when((core == 0) & (chip < chips - 1))
        def _():
            copy(chip, 1).start()

        copy(chip, 2).start()

    send_outward(tokens_copy)
    square_copy(0).start()
    loads["norm_gain"].wait()

    def share_info():
        loads["table"].wait()
        expert_ids = lax.broadcasted_iota(jnp.int32, (experts, rows), 0)
        table = jnp.zeros((experts, rows), jnp.float32)
        for choice in range(routes_ref.shape[0]):
            match = expert_ids == routes_ref[choice : choice + 1, :]
            table = table + jnp.where(match, weights_ref[choice : choice + 1, :], 0.0)
        info[ep, :experts] = table
        square_copy(0).wait_recv()
        square = square_out[0] + square_in[0]
        info[ep, experts:] = lax.rsqrt(square / (2 * width) + epsilon)
        send_outward(info_copy)

    def take(origin):
        tokens_copy(origin, 0).wait_recv()
        info_copy(origin, 0).wait_recv()
        pass_on(origin, 2)

    def toward_outer(origin):
        @pl.when(chip == 1)
        def _():
            pass_on(origin, 0)

        @pl.when(chip == chips - 2)
        def _():
            pass_on(origin, 1)

    def toward_inner(origin):
        @pl.when(chip < chips // 2)
        def _():
            pass_on(origin, 1)

        @pl.when(chip >= chips // 2)
        def _():
            pass_on(origin, 0)

    def relay(distance):
        @pl.when(chip >= distance)
        def _():
            take(chip - distance)

            @pl.when(chip < chips - 1)
            def _():
                pass_on(chip - distance, 1)

        @pl.when(chip + distance < chips)
        def _():
            take(chip + distance)

            @pl.when(chip > 0)
            def _():
                pass_on(chip + distance, 0)

    def second_lane_before(i):
        @pl.when((i == 4) & inner)
        def _():
            take(beyond)
            toward_outer(beyond)
            toward_outer(chip)

        @pl.when((i >= 4) & (i < 7) & outer)
        def _():
            take(origin_of(pick(i, slots)))

    def second_lane_after(i):
        @pl.when((i == 2) & inner)
        def _():
            take(beside)
            toward_inner(beside)
            toward_inner(chip)

        @pl.when((i == 3) & inner)
        def _():
            take(opposite)
            toward_outer(opposite)

    def locate(k):
        away_from = origin_of(pick(k, slots))
        origin = jnp.where((k == 0) | (k == other_at), chip, away_from)
        lane = jnp.where(core == 0, pick(k, lanes[0]), pick(k, lanes[1]))
        return origin, lane

    def block_of(k):
        origin, lane = locate(k)
        return origin * 2 + lane

    def scaled(block):
        source[...] = (held[block].astype(jnp.float32) * norm_gain_ref[...]).astype(jnp.bfloat16)

    def product_of(matrix, columns):
        return jnp.dot(
            source[...], matrix[columns], preferred_element_type=jnp.float32
        ).astype(jnp.bfloat16)

    def first_stage(k):
        origin, lane = locate(k)
        pl.when((k == 2) & (core == 0) & outer)(functools.partial(relay, 2))
        pl.when((k == 3) & (core == 0))(functools.partial(relay, 3))

        @pl.when(lane != core)
        def _():
            pair_gather_arrival(origin).wait_recv()

        scaled(block_of(k))
        pl.when(k == 0)(loads["gate_away"].wait)
        part_out[k, 0] = product_of(gate.at[0], (slice(None), away))
        part_copy(k, 0).start()

    def finish_first_stage(k):
        pl.when(k == 0)(loads["up_away"].wait)
        part_out[k, 1] = product_of(up.at[0], (slice(None), away))
        part_copy(k, 1).start()
        pl.when(k == 0)(loads["near"].wait)
        for which, matrix in enumerate((gate, up)):
            part_own[k, which] = product_of(matrix.at[0], (slice(None), near))

    def piece_of(side, piece):
        return pl.ds(pl.multiple_of(side * half + piece * quarter, quarter), quarter)

    def shared_first(piece):
        if piece == 0:
            loads["shared_in"].wait()
        else:
            scaled(ep)
        for side, target in ((1 - tp, part_out), (tp, part_own)):
            columns = (slice(None), piece_of(side, piece))
            for which, matrix in enumerate((gate, up)):
                place = slice(which * quarter, (which + 1) * quarter)
                target[shared_at, piece, :, place] = product_of(matrix.at[1], columns)
            if target is part_out:
                shared_part_copy(piece).start()

    def shared_second(piece):
        scale = across_lanes(unpack(info[ep, experts : experts + 1]), half)
        shared_part_copy(piece).wait_recv()
        total = part_own[shared_at, piece].astype(jnp.float32)
        total = (total + part_in[shared_at, piece].astype(jnp.float32)) * scale
        product_out = jax.nn.silu(total[:, :quarter]) * total[:, quarter:]
        place = slice(piece * quarter, (piece + 1) * quarter)
        hidden[shared_at, tp, :, place] = product_out.astype(jnp.bfloat16)
        shared_copy(piece, tp).start()

    def shared_product(piece, side, columns):
        place = slice(piece * quarter, (piece + 1) * quarter)
        return jnp.dot(
            hidden[shared_at, side, :, place],
            down[1, piece_of(side, piece), columns],
            preferred_element_type=jnp.float32,
        )

    def shared_third():
        def own_step(columns):
            mixture[:, columns] += shared_product(0, tp, columns)

        def other_step(columns):
            mixture[:, columns] += shared_product(0, 1 - tp, columns)

        tiles(own_step)
        shared_copy(0, 1 - tp).wait_recv()
        tiles(other_step)

    def second_stage(k):
        block = block_of(k)

        origin, lane = locate(k)

        @pl.when(lane != core)
        def _():
            pair_info_arrival(origin).wait_recv()

        scale = across_lanes(unpack(info[block, experts : experts + 1]), half)
        part_arrival(k).wait_recv()
        gate_sum = part_own[k, 0].astype(jnp.float32) + part_in[k, 0].astype(jnp.float32)
        up_sum = part_own[k, 1].astype(jnp.float32) + part_in[k, 1].astype(jnp.float32)
        gate_sum, up_sum = gate_sum * scale, up_sum * scale
        hidden[k, tp] = (jax.nn.silu(gate_sum) * up_sum).astype(jnp.bfloat16)
        hidden_copy(k, tp).start()

    def down_product(k, side, columns):
        rows_of = pl.ds(pl.multiple_of(side * half, half), half)
        return jnp.dot(
            hidden[k, side], down[0, rows_of, columns], preferred_element_type=jnp.float32
        )

    tile = width // 4

    def tiles(step, first=0, last=4):
        def tile_step(i, carry):
            step(pl.ds(pl.multiple_of(i * tile, tile), tile))
            return carry

        lax.fori_loop(first, last, tile_step, 0, unroll=last - first == 2)

    def third_stage(k):
        origin, lane = locate(k)
        pl.when(k == 0)(loads["down"].wait)

        def own_step(columns):
            product[:, columns] = down_product(k, tp, columns)

        keeper = lane == core
        kept = jnp.where(keeper, jnp.where(k == 0, MIXTURE, pick(k, slots)), SPARE)
        sent = jnp.where(keeper, chips, origin)

        def other_step(columns):
            total = product[:, columns] + down_product(k, 1 - tp, columns)
            weighted = total.astype(jnp.bfloat16).astype(jnp.float32) * scale
            sums[kept, :, columns] = weighted
            pair_out[sent, :, columns] = weighted.astype(jnp.bfloat16)

        tiles(own_step, 0, 4)
        scale = across_lanes(unpack(info[block_of(k), pl.ds(ep, 1)]), tile)
        hidden_copy(k, 1 - tp).wait_recv()
        for piece in range(2):
            tiles(other_step, 2 * piece, 2 * piece + 2)

            @pl.when(lane != core)
            def _(piece=piece):
                pair_copy(origin, piece).start()

    def fourth_stage(k):
        origin, lane = locate(k)

        @pl.when((k != 0) & (lane == core))
        def _():
            slot = pick(k, slots)
            direct = outer | (slot == NEAR)
            for piece in range(2):
                columns = part_of(piece)
                pair_copy(origin, piece).wait_recv()
                total = sums[slot, :, columns] + pair_in[origin, :, columns].astype(jnp.float32)
                sums[slot, :, columns] = total
                far_out[slot, :, columns] = total.astype(jnp.bfloat16)

                @pl.when(direct & (outer | (k != 1)))
                def _(piece=piece):
                    far_copy(slot, piece).start()

    def fifth_stage(k):
        slot = pick(k, slots)
        for piece in range(2):
            columns = part_of(piece)
            far_arrival(slot, piece).wait_recv()
            total = sums[slot, :, columns] + far_in[slot, :, columns].astype(jnp.float32)
            far_out[slot, :, columns] = total.astype(jnp.bfloat16)
            far_copy(slot, piece).start()

    def shared_own(columns):
        mixture[:, columns] += shared_product(1, tp, columns)

    def body(i, carry):
        early, late = i <= 3, (i >= 4) & (i <= count)
        pl.when(core == 1)(functools.partial(second_lane_before, i))

        @pl.when(i == 4)
        def _():
            fourth_stage(1)

        @pl.when((i == 6) & (core == 0) & inner)
        def _():
            far_copy(NEAR, 0).start()
            far_copy(NEAR, 1).start()

        @pl.when(i == 1)
        def _():
            pl.when(core == 0)(functools.partial(relay, 1))
            second_stage(0)
            pl.when((core == 1) & outer)(functools.partial(toward_inner, chip))

        @pl.when(i < count)
        def _():
            first_stage(i)

        @pl.when(i == count)
        def _():
            shared_first(1)

        @pl.when(early)
        def _():
            finish_first_stage(i)

        pl.when(core == 1)(functools.partial(second_lane_after, i))

        @pl.when(i == 0)
        def _():
            share_info()
            shared_first(0)

        @pl.when(i == 1)
        def _():
            shared_second(0)

        @pl.when(late)
        def _():
            third_stage(i - 2)

        pl.when((i == 2) & (core == 0) & inner)(functools.partial(relay, 2))

        @pl.when((i >= 2) & (i <= count))
        def _():
            second_stage(i - 1)

        @pl.when(late)
        def _():
            fourth_stage(i - 2)

        @pl.when(late & (i < count))
        def _():
            finish_first_stage(i)

        @pl.when(inner & jnp.where(core == 0, (i == 5) | (i == 6), (i == 7) | (i == 8)))
        def _():
            fifth_stage(i - 3)

        @pl.when(i == count + 1)
        def _():
            shared_second(1)
            tiles(shared_own)

        @pl.when((i == 2) | (i == 3) | (i == count + 1))
        def _():
            third_stage(i - 2)

        pl.when(i == 3)(shared_third)
        return carry

    lax.fori_loop(0, count + 2, body, 0)

    for piece in range(2):
        pair_copy(chip, piece).wait_recv()
        far_arrival(FAR + 1, piece).wait_recv()
        far_arrival(NEAR, piece).wait_recv()
    shared_copy(1, 1 - tp).wait_recv()
    squares = jnp.zeros((rows, 128), jnp.float32)
    for start in range(0, width, tile):
        columns = slice(start, start + tile)
        mixed = mixture[:, columns] + shared_product(1, 1 - tp, columns)
        for arrived in (pair_in.at[chip], far_in.at[FAR + 1], far_in.at[NEAR]):
            mixed = mixed + arrived[:, columns].astype(jnp.float32)
        mixture[:, columns] = mixed
        squares = squares + row_squares(mixed)
    square_out[1] = pack(squares)
    square_copy(1).start()
    loads["out_gain"].wait()
    mixture[...] *= out_gain_ref[...]
    square_copy(0).wait_send()
    square_copy(1).wait_send()

    def sent(whole, sem):
        pltpu.make_async_copy(whole, whole, sem.at[0]).wait()

    for whole, sem in ((held, gather_send), (info, info_send)):

        @pl.when(outer)
        def _(whole=whole, sem=sem):
            pltpu.make_async_copy(whole.at[0], whole.at[0], sem.at[0]).wait()

        @pl.when(inner)
        def _(whole=whole, sem=sem):
            several = whole.at[: chips + 1]
            pltpu.make_async_copy(several, several, sem.at[0]).wait()

        pltpu.make_async_copy(whole.at[:chips], whole.at[:chips], sem.at[1]).wait()

    sent(part_out, part_send)
    sent(part_out.at[:, 0], hidden_send)
    sent(pair_in, pair_send)
    sent(far_out, far_send)
    square_copy(1).wait_recv()
    scale = lax.rsqrt(unpack(square_out[1] + square_in[1]) / (2 * width) + epsilon)
    out_ref[...] = (mixture[...] * across_lanes(scale, width)).astype(jnp.bfloat16)


def fused(
    chips,
    tokens,
    routes,
    route_weights,
    norm_gain,
    expert_gate,
    expert_up,
    expert_down,
    shared_gate,
    shared_up,
    shared_down,
    out_gain,
):
    rows, width = tokens.shape
    units = shared_gate.shape[1]
    half = units // 2
    count = 2 * chips + 1
    choices = routes.shape[1]
    vmem = pl.BlockSpec(memory_space=pltpu.VMEM)
    hbm = pl.BlockSpec(memory_space=pl.ANY)
    bf16, f32 = jnp.bfloat16, jnp.float32
    dma = pltpu.SemaphoreType.DMA
    return pl.pallas_call(
        functools.partial(fused_kernel, chips),
        out_shape=pltpu.VMEM((rows, width), bf16),
        in_specs=[hbm] * 11,
        out_specs=vmem,
        scratch_shapes=[
            pltpu.VMEM((choices, rows), jnp.int32),
            pltpu.VMEM((choices, rows), f32),
            pltpu.VMEM((1, width), f32),
            pltpu.VMEM((1, width), f32),
            pltpu.VMEM((2, width, units), bf16),
            pltpu.VMEM((2, width, units), bf16),
            pltpu.VMEM((2, units, width), bf16),
            pltpu.VMEM((2 * chips, rows, width), bf16),
            pltpu.VMEM((rows, width), bf16),
            pltpu.VMEM((count, 2, rows, half), bf16),
            pltpu.VMEM((count, 2, rows, half), bf16),
            pltpu.VMEM((count, 2, rows, half), bf16),
            pltpu.VMEM((count, 2, rows, half), bf16),
            pltpu.VMEM((rows, width), f32),
            pltpu.VMEM((5, rows, width), f32),
            pltpu.VMEM((chips + 1, rows, width), bf16),
            pltpu.VMEM((chips, rows, width), bf16),
            pltpu.VMEM((3, rows, width), bf16),
            pltpu.VMEM((4, rows, width), bf16),
            pltpu.VMEM((2, 8, rows), f32),
            pltpu.VMEM((2, 8, rows), f32),
            pltpu.VMEM((2 * chips, 2 * chips + 8, rows), f32),
            dma((9,)),
            dma((2,)),
            dma((chips,)),
            dma((chips,)),
            dma((2,)),
            dma((2,)),
            dma((2,)),
            dma((chips,)),
            dma((chips,)),
            dma((1,)),
            dma((5,)),
            dma((1,)),
            dma((6,)),
            dma((1,)),
            dma((chips, 2)),
            dma((1,)),
            dma((4, 2)),
        ],
        compiler_params=pltpu.CompilerParams(
            collective_id=0, has_side_effects=True, vmem_limit_bytes=60 * 1024 * 1024
        ),
    )(
        tokens,
        routes.T,
        route_weights.T,
        norm_gain.reshape(1, -1),
        expert_gate,
        expert_up,
        expert_down,
        shared_gate,
        shared_up,
        shared_down,
        out_gain.reshape(1, -1),
    )


def local_product(source, matrix):
    return jnp.dot(source, matrix, preferred_element_type=jnp.float32)


def per_device(
    tokens,
    routes,
    route_weights,
    norm_gain,
    expert_gate,
    expert_up,
    expert_down,
    shared_gate,
    shared_up,
    shared_down,
    out_gain,
):
    block_width = tokens.shape[1]
    full_width = block_width * lax.axis_size("tp")
    width_index = lax.axis_index("tp")
    full_rows = lax.all_gather(tokens, "tp", axis=1, tiled=True)
    full_float = full_rows.astype(jnp.float32)
    normed_full = (
        full_float
        * lax.rsqrt(jnp.mean(full_float * full_float, axis=-1, keepdims=True) + epsilon)
        * norm_gain
    ).astype(jnp.bfloat16)
    normed_block = lax.dynamic_slice_in_dim(normed_full, width_index * block_width, block_width, 1)
    gate_matrix = expert_gate[0]
    up_matrix = expert_up[0]
    down_matrix = expert_down[0]
    experts = lax.axis_size("ep")
    choose = (routes[:, :, None] == jnp.arange(experts, dtype=jnp.int32)[None, None, :]).astype(
        jnp.float32
    )
    weight_table = jnp.sum(route_weights[:, :, None] * choose, axis=1)
    expert_input = lax.all_gather(normed_block, "ep", axis=0, tiled=True)
    table_all = lax.all_gather(weight_table, "ep", axis=0, tiled=True)
    summed = (
        lax.psum(local_product(expert_input, gate_matrix).astype(jnp.bfloat16), "tp").astype(
            jnp.float32
        ),
        lax.psum(local_product(expert_input, up_matrix).astype(jnp.bfloat16), "tp").astype(
            jnp.float32
        ),
        lax.psum(local_product(normed_block, shared_gate).astype(jnp.bfloat16), "tp").astype(
            jnp.float32
        ),
        lax.psum(local_product(normed_block, shared_up).astype(jnp.bfloat16), "tp").astype(
            jnp.float32
        ),
    )
    routed_hidden = (jax.nn.silu(summed[0]) * summed[1]).astype(jnp.bfloat16)
    shared_hidden = (jax.nn.silu(summed[2]) * summed[3]).astype(jnp.bfloat16)
    expert_rows = local_product(routed_hidden, down_matrix).astype(jnp.bfloat16)
    shared_out = local_product(shared_hidden, shared_down)
    own_expert = lax.axis_index("ep")
    column = lax.dynamic_slice_in_dim(table_all, own_expert, 1, 1)
    routed = lax.psum_scatter(
        (column * expert_rows.astype(jnp.float32)).astype(jnp.bfloat16),
        "ep",
        scatter_dimension=0,
        tiled=True,
    ).astype(jnp.float32)
    mixture = routed + shared_out
    square_sum = lax.psum(jnp.sum(mixture * mixture, axis=-1, keepdims=True), "tp")
    scale = lax.rsqrt(square_sum / full_width + epsilon)
    return (mixture * scale * out_gain).astype(jnp.bfloat16)


def solution(mesh):
    chips = mesh.shape["ep"] // 2
    if mesh.shape["tp"] == 2 and mesh.shape["ep"] == 8:
        body = functools.partial(fused, chips)
    else:
        body = per_device
    return jax.shard_map(
        body,
        mesh=mesh,
        in_specs=(
            P(("grp", "ep"), "tp"),
            P(("grp", "ep"), None),
            P(("grp", "ep"), None),
            P(),
            P("ep", "tp", None),
            P("ep", "tp", None),
            P("ep", None, "tp"),
            P("tp", None),
            P("tp", None),
            P(None, "tp"),
            P("tp"),
        ),
        out_specs=P(("grp", "ep"), "tp"),
        check_vma=False,
    )
```

```python
import functools

import jax
import jax.numpy as jnp
from jax import lax
from jax.experimental import pallas as pl
from jax.experimental.pallas import tpu as pltpu
from jax.sharding import PartitionSpec as P

epsilon = 1e-06
MESH = pl.DeviceIdType.MESH


NEAR, MIDDLE, FAR, SPARE, MIXTURE = range(5)
STEPS = (
    "own",
    (NEAR, 0),
    (MIDDLE, 0),
    (FAR, 0),
    (FAR, 1),
    (MIDDLE, 1),
    (NEAR, 1),
    "other",
)


def pick(index, table):
    value = jnp.int32(table[0])
    for position in range(1, len(table)):
        if table[position] != table[0]:
            value = jnp.where(index == position, jnp.int32(table[position]), value)
    return value


def exclusive_or(a, b, size):
    total, unit = jnp.int32(0), 1
    while unit < size:
        total = total + unit * lax.rem(lax.div(a, unit) + lax.div(b, unit), 2)
        unit *= 2
    return total


def fused_kernel(
    chips,
    tokens_hbm,
    routes_hbm,
    weights_hbm,
    norm_gain_hbm,
    gate_hbm,
    up_hbm,
    down_hbm,
    shared_gate_hbm,
    shared_up_hbm,
    shared_down_hbm,
    out_gain_hbm,
    out_ref,
    routes_ref,
    weights_ref,
    norm_gain_ref,
    out_gain_ref,
    gate,
    up,
    down,
    held,
    source,
    part_out,
    part_in,
    part_own,
    hidden,
    product,
    sums,
    pair_out,
    pair_in,
    far_out,
    far_in,
    square_out,
    square_in,
    info,
    load_sem,
    info_send,
    info_recv,
    pair_info_recv,
    square_send,
    square_recv,
    gather_send,
    gather_recv,
    pair_gather_recv,
    part_send,
    part_recv,
    hidden_send,
    hidden_recv,
    pair_send,
    pair_recv,
    far_send,
    far_recv,
):
    rows, width = product.shape
    mixture = sums.at[MIXTURE]
    experts = 2 * chips
    units = gate.shape[2]
    half = units // 2
    count = len(STEPS)
    slots = [step[0] if isinstance(step, tuple) else NEAR for step in STEPS]
    lanes = [
        [side if step == "own" else 1 - side if step == "other" else step[1] if isinstance(step, tuple) else side for step in STEPS]
        for side in range(2)
    ]
    cuts = [0, half // 4, half]
    spans = [slice(cuts[piece], cuts[piece + 1]) for piece in range(2)]
    other_at, shared_at = count - 1, count

    ep = lax.axis_index("ep")
    tp = lax.axis_index("tp")
    chip, core = lax.div(ep, 2), 1 - lax.rem(ep, 2)
    other_core = 1 - core
    partner = {"ep": chip * 2 + core}
    me = chip * 2 + core

    def same_core(place):
        return {"ep": place * 2 + other_core}

    across = {"tp": 1 - tp}

    away = pl.ds(pl.multiple_of((1 - tp) * half, half), half)
    near = pl.ds(pl.multiple_of(tp * half, half), half)
    features = pl.ds(pl.multiple_of(tp * width, width), width)
    groups = [
        [(tokens_hbm, held.at[me])],
        [(norm_gain_hbm.at[:, features], norm_gain_ref)],
        [(gate_hbm.at[0, :, away], gate.at[0, :, away])],
        [(up_hbm.at[0, :, away], up.at[0, :, away])],
        [
            (gate_hbm.at[0, :, near], gate.at[0, :, near]),
            (up_hbm.at[0, :, near], up.at[0, :, near]),
        ],
        [(routes_hbm, routes_ref), (weights_hbm, weights_ref)],
        [(shared_gate_hbm, gate.at[1]), (shared_up_hbm, up.at[1])],
        [(down_hbm.at[0], down.at[0]), (shared_down_hbm, down.at[1])],
        [(out_gain_hbm, out_gain_ref)],
    ]
    wholes = [held.at[me], norm_gain_ref, gate.at[0, :, away], up.at[0, :, away]]
    wholes += [gate.at[0], info.at[0, :8], gate, down, out_gain_ref]
    names = ["tokens", "norm_gain", "gate_away", "up_away", "near", "table"]
    names += ["shared_in", "down", "out_gain"]

    loads = {
        name: pltpu.make_async_copy(whole, whole, load_sem.at[i])
        for i, (name, whole) in enumerate(zip(names, wholes))
    }
    for i, group in enumerate(groups):
        for load_from, load_to in group:
            pltpu.make_async_copy(load_from, load_to, load_sem.at[i]).start()

    barrier = pltpu.get_barrier_semaphore()
    def greet(device):
        pl.semaphore_signal(barrier, inc=1, device_id=device, device_id_type=MESH)

    greet(across)
    greet(partner)

    @pl.when(chip > 0)
    def _():
        greet(same_core(chip - 1))

    @pl.when(chip < chips - 1)
    def _():
        greet(same_core(chip + 1))

    def remote(source, target, send, recv, device):
        return pltpu.make_async_remote_copy(
            src_ref=source,
            dst_ref=target,
            send_sem=send,
            recv_sem=recv,
            device_id=device,
            device_id_type=MESH,
        )

    def square_copy(which):
        return remote(
            square_out.at[which],
            square_in.at[which],
            square_send.at[which],
            square_recv.at[which],
            across,
        )

    def ways(way):
        return (same_core(chip - 1), same_core(chip + 1), partner)[way]

    def tokens_copy(origin, way):
        slot = held.at[origin * 2 + core]
        recv = (pair_gather_recv if way == 2 else gather_recv).at[origin]
        return remote(slot, slot, gather_send.at[way // 2], recv, ways(way))

    def info_copy(origin, way):
        slot = info.at[origin * 2 + core]
        recv = (pair_info_recv if way == 2 else info_recv).at[origin]
        return remote(slot, slot, info_send.at[way // 2], recv, ways(way))

    def pass_on(origin, way):
        tokens_copy(origin, way).start()
        info_copy(origin, way).start()

    def pair_info_arrival(origin):
        slot = info.at[origin * 2 + other_core]
        return remote(slot, slot, info_send.at[1], pair_info_recv.at[origin], partner)

    def pair_gather_arrival(origin):
        slot = held.at[origin * 2 + other_core]
        return remote(slot, slot, gather_send.at[1], pair_gather_recv.at[origin], partner)

    def part_copy(k, which):
        place = lax.rem(k, 3)
        return remote(
            part_out.at[k, which],
            part_in.at[k, which],
            part_send.at[0],
            part_recv.at[place],
            across,
        )

    def part_arrival(k):
        place = lax.rem(k, 3)
        return remote(
            part_out.at[k], part_in.at[k], part_send.at[0], part_recv.at[place], across
        )

    def shared_part_copy(piece, which):
        return remote(
            part_out.at[shared_at, which, :, spans[piece]],
            part_in.at[shared_at, which, :, spans[piece]],
            part_send.at[0],
            part_recv.at[3 + piece],
            across,
        )

    def shared_part_arrival(piece):
        return remote(
            part_out.at[shared_at, :, :, spans[piece]],
            part_in.at[shared_at, :, :, spans[piece]],
            part_send.at[0],
            part_recv.at[3 + piece],
            across,
        )

    def hidden_copy(k, side):
        slot = hidden.at[k, side]
        return remote(slot, slot, hidden_send.at[0], hidden_recv.at[lax.rem(k, 4)], across)

    def shared_copy(piece, side):
        slot = hidden.at[shared_at, side, :, spans[piece]]
        return remote(slot, slot, hidden_send.at[0], hidden_recv.at[4 + piece], across)

    def part_of(piece):
        return pl.ds(piece * (width // 2), width // 2)

    def pair_copy(origin, piece):
        return remote(
            pair_out.at[origin, :, part_of(piece)],
            pair_in.at[origin, :, part_of(piece)],
            pair_send.at[0],
            pair_recv.at[origin, piece],
            partner,
        )

    beside, opposite, beyond = (exclusive_or(chip, mask, chips) for mask in (1, 2, 3))
    outer = (chip == 0) | (chip == chips - 1)
    inner = jnp.logical_not(outer)

    def origin_of(slot):
        middle, far = jnp.where(outer, opposite, beyond), jnp.where(outer, beyond, opposite)
        return jnp.where(slot == NEAR, beside, jnp.where(slot == MIDDLE, middle, far))

    def far_copy(slot, piece):
        direct = outer | (slot == NEAR)
        place = jnp.where(direct, slot, FAR + 1)
        target = jnp.where(direct, beside, origin_of(slot))
        return remote(
            far_out.at[slot, :, part_of(piece)],
            far_in.at[place, :, part_of(piece)],
            far_send.at[0],
            far_recv.at[place, piece],
            same_core(target),
        )

    def far_arrival(place, piece):
        return remote(
            far_out.at[0, :, part_of(piece)],
            far_in.at[place, :, part_of(piece)],
            far_send.at[0],
            far_recv.at[place, piece],
            same_core(beside),
        )

    def row_squares(values):
        total = jnp.zeros((rows, 128), jnp.float32)
        for start in range(0, values.shape[1], 128):
            chunk = values[:, start : start + 128]
            total = total + chunk * chunk
        return total

    def pack(partial):
        row = jnp.sum(jnp.transpose(partial), axis=0, keepdims=True)
        return jnp.broadcast_to(row, (8, rows))

    def unpack(row):
        return jnp.transpose(jnp.broadcast_to(row[:1], (128, rows)))

    def across_lanes(column, lanes):
        return jnp.concatenate([column] * (lanes // 128), axis=1)

    loads["tokens"].wait()
    def scaled(block):
        source[...] = (held[block].astype(jnp.float32) * norm_gain_ref[...]).astype(jnp.bfloat16)

    def product_of(matrix, columns):
        return jnp.dot(
            source[...], matrix[columns], preferred_element_type=jnp.float32
        ).astype(jnp.bfloat16)

    def first_gate():
        loads["gate_away"].wait()
        part_out[0, 0] = product_of(gate.at[0], (slice(None), away))

    square_out[0] = pack(row_squares(held[me].astype(jnp.float32)))
    loads["norm_gain"].wait()
    ahead = chip == 0

    @pl.when(ahead)
    def _():
        scaled(me)
        first_gate()

    pl.semaphore_wait(barrier, jnp.where((chip == 0) | (chip == chips - 1), 3, 4))

    def send_outward(copy):
        @pl.when((core == 0) & (chip > 0))
        def _():
            copy(chip, 0).start()

        @pl.when((core == 0) & (chip < chips - 1))
        def _():
            copy(chip, 1).start()

        copy(chip, 2).start()

    send_outward(tokens_copy)
    square_copy(0).start()

    def share_info():
        loads["table"].wait()
        expert_ids = lax.broadcasted_iota(jnp.int32, (experts, rows), 0)
        table = jnp.zeros((experts, rows), jnp.float32)
        for choice in range(routes_ref.shape[0]):
            match = expert_ids == routes_ref[choice : choice + 1, :]
            table = table + jnp.where(match, weights_ref[choice : choice + 1, :], 0.0)
        info[me, :experts] = table
        square_copy(0).wait_recv()
        square = square_out[0] + square_in[0]
        info[me, experts:] = lax.rsqrt(square / (2 * width) + epsilon)
        send_outward(info_copy)

    def take(origin):
        tokens_copy(origin, 0).wait_recv()
        info_copy(origin, 0).wait_recv()
        pass_on(origin, 2)

    def toward_outer(origin):
        @pl.when(chip == 1)
        def _():
            pass_on(origin, 0)

        @pl.when(chip == chips - 2)
        def _():
            pass_on(origin, 1)

    def toward_inner(origin):
        @pl.when(chip < chips // 2)
        def _():
            pass_on(origin, 1)

        @pl.when(chip >= chips // 2)
        def _():
            pass_on(origin, 0)

    def relay(distance):
        @pl.when(chip >= distance)
        def _():
            take(chip - distance)

            @pl.when(chip < chips - 1)
            def _():
                pass_on(chip - distance, 1)

        @pl.when(chip + distance < chips)
        def _():
            take(chip + distance)

            @pl.when(chip > 0)
            def _():
                pass_on(chip + distance, 0)

    def second_lane_before(i):
        @pl.when((i == 4) & inner)
        def _():
            take(beyond)
            toward_outer(beyond)
            toward_outer(chip)

        @pl.when((i >= 4) & (i < 7) & outer)
        def _():
            take(origin_of(pick(i, slots)))

    def second_lane_after(i):
        @pl.when((i == 2) & inner)
        def _():
            take(beside)
            toward_inner(beside)
            toward_inner(chip)

        @pl.when((i == 3) & inner)
        def _():
            take(opposite)
            toward_outer(opposite)

    def locate(k):
        away_from = origin_of(pick(k, slots))
        origin = jnp.where((k == 0) | (k == other_at), chip, away_from)
        lane = jnp.where(core == 0, pick(k, lanes[0]), pick(k, lanes[1]))
        return origin, lane

    def block_of(k):
        origin, lane = locate(k)
        return origin * 2 + lane

    def first_stage(k):
        origin, lane = locate(k)
        pl.when((k == 2) & (core == 0) & outer)(functools.partial(relay, 2))
        pl.when((k == 3) & (core == 0))(functools.partial(relay, 3))

        @pl.when(lane != core)
        def _():
            pair_gather_arrival(origin).wait_recv()

        pl.when((k == 0) & jnp.logical_not(ahead))(loads["gate_away"].wait)

        @pl.when((k != 0) | jnp.logical_not(ahead))
        def _():
            scaled(block_of(k))
            part_out[k, 0] = product_of(gate.at[0], (slice(None), away))

        part_copy(k, 0).start()

    def finish_first_stage(k):
        pl.when(k == 0)(loads["up_away"].wait)
        part_out[k, 1] = product_of(up.at[0], (slice(None), away))
        part_copy(k, 1).start()
        pl.when(k == 0)(loads["near"].wait)
        for which, matrix in enumerate((gate, up)):
            part_own[k, which] = product_of(matrix.at[0], (slice(None), near))

    def piece_of(side, piece):
        start = pl.multiple_of(side * half + cuts[piece], half // 4)
        return pl.ds(start, cuts[piece + 1] - cuts[piece])

    def shared_first(piece):
        if piece == 0:
            loads["shared_in"].wait()
        else:
            scaled(me)
        for side, target in ((1 - tp, part_out), (tp, part_own)):
            columns = (slice(None), piece_of(side, piece))
            for which, matrix in enumerate((gate, up)):
                target[shared_at, which, :, spans[piece]] = product_of(matrix.at[1], columns)
                if target is part_out:
                    shared_part_copy(piece, which).start()

    def shared_second(piece):
        scale = unpack(info[me, experts : experts + 1])
        scale = across_lanes(scale, cuts[piece + 1] - cuts[piece])
        shared_part_arrival(piece).wait_recv()

        def total(which):
            own = part_own[shared_at, which, :, spans[piece]].astype(jnp.float32)
            return (own + part_in[shared_at, which, :, spans[piece]].astype(jnp.float32)) * scale

        product_out = jax.nn.silu(total(0)) * total(1)
        hidden[shared_at, tp, :, spans[piece]] = product_out.astype(jnp.bfloat16)
        shared_copy(piece, tp).start()

    def shared_product(piece, side, columns):
        return jnp.dot(
            hidden[shared_at, side, :, spans[piece]],
            down[1, piece_of(side, piece), columns],
            preferred_element_type=jnp.float32,
        )

    def shared_third():
        def own_step(columns):
            mixture[:, columns] += shared_product(0, tp, columns)

        def other_step(columns):
            mixture[:, columns] += shared_product(0, 1 - tp, columns)

        tiles(own_step)
        shared_copy(0, 1 - tp).wait_recv()
        tiles(other_step)

    def second_stage(k):
        block = block_of(k)

        origin, lane = locate(k)

        @pl.when(lane != core)
        def _():
            pair_info_arrival(origin).wait_recv()

        scale = across_lanes(unpack(info[block, experts : experts + 1]), half)
        part_arrival(k).wait_recv()
        gate_sum = part_own[k, 0].astype(jnp.float32) + part_in[k, 0].astype(jnp.float32)
        up_sum = part_own[k, 1].astype(jnp.float32) + part_in[k, 1].astype(jnp.float32)
        gate_sum, up_sum = gate_sum * scale, up_sum * scale
        hidden[k, tp] = (jax.nn.silu(gate_sum) * up_sum).astype(jnp.bfloat16)
        hidden_copy(k, tp).start()

    def down_product(k, side, columns):
        rows_of = pl.ds(pl.multiple_of(side * half, half), half)
        return jnp.dot(
            hidden[k, side], down[0, rows_of, columns], preferred_element_type=jnp.float32
        )

    tile = width // 4

    def tiles(step, first=0, last=4):
        def tile_step(i, carry):
            step(pl.ds(pl.multiple_of(i * tile, tile), tile))
            return carry

        lax.fori_loop(first, last, tile_step, 0, unroll=last - first == 2)

    def third_stage(k):
        origin, lane = locate(k)
        pl.when(k == 0)(loads["down"].wait)

        def own_step(columns):
            product[:, columns] = down_product(k, tp, columns)

        keeper = lane == core
        kept = jnp.where(keeper, jnp.where(k == 0, MIXTURE, pick(k, slots)), SPARE)
        sent = jnp.where(keeper, chips, origin)

        def other_step(columns):
            total = product[:, columns] + down_product(k, 1 - tp, columns)
            weighted = total.astype(jnp.bfloat16).astype(jnp.float32) * scale
            sums[kept, :, columns] = weighted
            pair_out[sent, :, columns] = weighted.astype(jnp.bfloat16)

        tiles(own_step, 0, 4)
        scale = across_lanes(unpack(info[block_of(k), pl.ds(ep, 1)]), tile)
        hidden_copy(k, 1 - tp).wait_recv()
        for piece in range(2):
            tiles(other_step, 2 * piece, 2 * piece + 2)

            @pl.when(lane != core)
            def _(piece=piece):
                pair_copy(origin, piece).start()

    def fourth_stage(k):
        origin, lane = locate(k)

        @pl.when((k != 0) & (lane == core))
        def _():
            slot = pick(k, slots)
            direct = outer | (slot == NEAR)
            for piece in range(2):
                columns = part_of(piece)
                pair_copy(origin, piece).wait_recv()
                total = sums[slot, :, columns] + pair_in[origin, :, columns].astype(jnp.float32)
                sums[slot, :, columns] = total
                far_out[slot, :, columns] = total.astype(jnp.bfloat16)

                @pl.when(direct & (outer | (k != 1)))
                def _(piece=piece):
                    far_copy(slot, piece).start()

    def fifth_stage(k):
        slot = pick(k, slots)
        for piece in range(2):
            columns = part_of(piece)
            far_arrival(slot, piece).wait_recv()
            total = sums[slot, :, columns] + far_in[slot, :, columns].astype(jnp.float32)
            far_out[slot, :, columns] = total.astype(jnp.bfloat16)
            far_copy(slot, piece).start()

    def shared_own(columns):
        mixture[:, columns] += shared_product(1, tp, columns)

    def body(i, carry):
        early, late = i <= 3, (i >= 4) & (i <= count)
        pl.when(core == 1)(functools.partial(second_lane_before, i))

        @pl.when(i == 4)
        def _():
            fourth_stage(1)

        @pl.when((i == 6) & (core == 0) & inner)
        def _():
            far_copy(NEAR, 0).start()
            far_copy(NEAR, 1).start()

        @pl.when(i == 1)
        def _():
            pl.when(core == 0)(functools.partial(relay, 1))
            second_stage(0)

        @pl.when(i < count)
        def _():
            first_stage(i)

        @pl.when(i == count)
        def _():
            shared_first(1)

        @pl.when(early)
        def _():
            finish_first_stage(i)

        pl.when(core == 1)(functools.partial(second_lane_after, i))

        @pl.when(i == 0)
        def _():
            share_info()
            shared_first(0)
            pl.when((core == 1) & outer)(functools.partial(toward_inner, chip))

        @pl.when(i == 1)
        def _():
            shared_second(0)

        @pl.when(late)
        def _():
            third_stage(i - 2)

        pl.when((i == 2) & (core == 0) & inner)(functools.partial(relay, 2))

        @pl.when((i >= 2) & (i <= count))
        def _():
            second_stage(i - 1)

        @pl.when(late)
        def _():
            fourth_stage(i - 2)

        @pl.when(late & (i < count))
        def _():
            finish_first_stage(i)

        @pl.when(inner & jnp.where(core == 0, (i == 5) | (i == 6), (i == 7) | (i == 8)))
        def _():
            fifth_stage(i - 3)

        @pl.when(i == count + 1)
        def _():
            shared_second(1)
            tiles(shared_own)

        @pl.when((i == 2) | (i == 3) | (i == count + 1))
        def _():
            third_stage(i - 2)

        pl.when(i == 3)(shared_third)
        return carry

    lax.fori_loop(0, count + 2, body, 0)

    def shared_other(columns):
        mixture[:, columns] += shared_product(1, 1 - tp, columns)

    shared_copy(1, 1 - tp).wait_recv()
    tiles(shared_other, 0, 2)
    tiles(shared_other, 2, 4)
    squares = jnp.zeros((rows, 128), jnp.float32)
    for piece in range(2):
        pair_copy(chip, piece).wait_recv()
        far_arrival(FAR + 1, piece).wait_recv()
        far_arrival(NEAR, piece).wait_recv()
        for start in range(piece * width // 2, (piece + 1) * width // 2, tile):
            columns = slice(start, start + tile)
            mixed = mixture[:, columns]
            for arrived in (pair_in.at[chip], far_in.at[FAR + 1], far_in.at[NEAR]):
                mixed = mixed + arrived[:, columns].astype(jnp.float32)
            mixture[:, columns] = mixed
            squares = squares + row_squares(mixed)
    square_out[1] = pack(squares)
    square_copy(1).start()
    loads["out_gain"].wait()
    mixture[...] *= out_gain_ref[...]
    square_copy(0).wait_send()
    square_copy(1).wait_send()

    def sent(whole, sem):
        pltpu.make_async_copy(whole, whole, sem.at[0]).wait()

    for whole, sem in ((held, gather_send), (info, info_send)):

        @pl.when(outer)
        def _(whole=whole, sem=sem):
            pltpu.make_async_copy(whole.at[0], whole.at[0], sem.at[0]).wait()

        @pl.when(inner)
        def _(whole=whole, sem=sem):
            several = whole.at[: chips + 1]
            pltpu.make_async_copy(several, several, sem.at[0]).wait()

        pltpu.make_async_copy(whole.at[:chips], whole.at[:chips], sem.at[1]).wait()

    sent(part_out, part_send)
    sent(part_out.at[:, 0], hidden_send)
    sent(pair_in, pair_send)
    sent(far_out, far_send)
    square_copy(1).wait_recv()
    scale = lax.rsqrt(unpack(square_out[1] + square_in[1]) / (2 * width) + epsilon)
    out_ref[...] = (mixture[...] * across_lanes(scale, width)).astype(jnp.bfloat16)


def fused(
    chips,
    tokens,
    routes,
    route_weights,
    norm_gain,
    expert_gate,
    expert_up,
    expert_down,
    shared_gate,
    shared_up,
    shared_down,
    out_gain,
):
    rows, width = tokens.shape
    units = shared_gate.shape[1]
    half = units // 2
    count = 2 * chips + 1
    choices = routes.shape[1]
    vmem = pl.BlockSpec(memory_space=pltpu.VMEM)
    hbm = pl.BlockSpec(memory_space=pl.ANY)
    bf16, f32 = jnp.bfloat16, jnp.float32
    dma = pltpu.SemaphoreType.DMA
    return pl.pallas_call(
        functools.partial(fused_kernel, chips),
        out_shape=pltpu.VMEM((rows, width), bf16),
        in_specs=[hbm] * 11,
        out_specs=vmem,
        scratch_shapes=[
            pltpu.VMEM((choices, rows), jnp.int32),
            pltpu.VMEM((choices, rows), f32),
            pltpu.VMEM((1, width), f32),
            pltpu.VMEM((1, width), f32),
            pltpu.VMEM((2, width, units), bf16),
            pltpu.VMEM((2, width, units), bf16),
            pltpu.VMEM((2, units, width), bf16),
            pltpu.VMEM((2 * chips, rows, width), bf16),
            pltpu.VMEM((rows, width), bf16),
            pltpu.VMEM((count, 2, rows, half), bf16),
            pltpu.VMEM((count, 2, rows, half), bf16),
            pltpu.VMEM((count, 2, rows, half), bf16),
            pltpu.VMEM((count, 2, rows, half), bf16),
            pltpu.VMEM((rows, width), f32),
            pltpu.VMEM((5, rows, width), f32),
            pltpu.VMEM((chips + 1, rows, width), bf16),
            pltpu.VMEM((chips, rows, width), bf16),
            pltpu.VMEM((3, rows, width), bf16),
            pltpu.VMEM((4, rows, width), bf16),
            pltpu.VMEM((2, 8, rows), f32),
            pltpu.VMEM((2, 8, rows), f32),
            pltpu.VMEM((2 * chips, 2 * chips + 8, rows), f32),
            dma((9,)),
            dma((2,)),
            dma((chips,)),
            dma((chips,)),
            dma((2,)),
            dma((2,)),
            dma((2,)),
            dma((chips,)),
            dma((chips,)),
            dma((1,)),
            dma((5,)),
            dma((1,)),
            dma((6,)),
            dma((1,)),
            dma((chips, 2)),
            dma((1,)),
            dma((4, 2)),
        ],
        compiler_params=pltpu.CompilerParams(
            collective_id=0, has_side_effects=True, vmem_limit_bytes=60 * 1024 * 1024
        ),
    )(
        tokens,
        routes.T,
        route_weights.T,
        norm_gain.reshape(1, -1),
        expert_gate,
        expert_up,
        expert_down,
        shared_gate,
        shared_up,
        shared_down,
        out_gain.reshape(1, -1),
    )


def local_product(source, matrix):
    return jnp.dot(source, matrix, preferred_element_type=jnp.float32)


def per_device(
    tokens,
    routes,
    route_weights,
    norm_gain,
    expert_gate,
    expert_up,
    expert_down,
    shared_gate,
    shared_up,
    shared_down,
    out_gain,
):
    block_width = tokens.shape[1]
    full_width = block_width * lax.axis_size("tp")
    width_index = lax.axis_index("tp")
    full_rows = lax.all_gather(tokens, "tp", axis=1, tiled=True)
    full_float = full_rows.astype(jnp.float32)
    normed_full = (
        full_float
        * lax.rsqrt(jnp.mean(full_float * full_float, axis=-1, keepdims=True) + epsilon)
        * norm_gain
    ).astype(jnp.bfloat16)
    normed_block = lax.dynamic_slice_in_dim(normed_full, width_index * block_width, block_width, 1)
    gate_matrix = expert_gate[0]
    up_matrix = expert_up[0]
    down_matrix = expert_down[0]
    experts = lax.axis_size("ep")
    choose = (routes[:, :, None] == jnp.arange(experts, dtype=jnp.int32)[None, None, :]).astype(
        jnp.float32
    )
    weight_table = jnp.sum(route_weights[:, :, None] * choose, axis=1)
    expert_input = lax.all_gather(normed_block, "ep", axis=0, tiled=True)
    table_all = lax.all_gather(weight_table, "ep", axis=0, tiled=True)
    summed = (
        lax.psum(local_product(expert_input, gate_matrix).astype(jnp.bfloat16), "tp").astype(
            jnp.float32
        ),
        lax.psum(local_product(expert_input, up_matrix).astype(jnp.bfloat16), "tp").astype(
            jnp.float32
        ),
        lax.psum(local_product(normed_block, shared_gate).astype(jnp.bfloat16), "tp").astype(
            jnp.float32
        ),
        lax.psum(local_product(normed_block, shared_up).astype(jnp.bfloat16), "tp").astype(
            jnp.float32
        ),
    )
    routed_hidden = (jax.nn.silu(summed[0]) * summed[1]).astype(jnp.bfloat16)
    shared_hidden = (jax.nn.silu(summed[2]) * summed[3]).astype(jnp.bfloat16)
    expert_rows = local_product(routed_hidden, down_matrix).astype(jnp.bfloat16)
    shared_out = local_product(shared_hidden, shared_down)
    own_expert = lax.axis_index("ep")
    column = lax.dynamic_slice_in_dim(table_all, own_expert, 1, 1)
    routed = lax.psum_scatter(
        (column * expert_rows.astype(jnp.float32)).astype(jnp.bfloat16),
        "ep",
        scatter_dimension=0,
        tiled=True,
    ).astype(jnp.float32)
    mixture = routed + shared_out
    square_sum = lax.psum(jnp.sum(mixture * mixture, axis=-1, keepdims=True), "tp")
    scale = lax.rsqrt(square_sum / full_width + epsilon)
    return (mixture * scale * out_gain).astype(jnp.bfloat16)


def solution(mesh):
    chips = mesh.shape["ep"] // 2
    if mesh.shape["tp"] == 2 and mesh.shape["ep"] == 8:
        body = functools.partial(fused, chips)
    else:
        body = per_device
    return jax.shard_map(
        body,
        mesh=mesh,
        in_specs=(
            P(("grp", "ep"), "tp"),
            P(("grp", "ep"), None),
            P(("grp", "ep"), None),
            P(),
            P("ep", "tp", None),
            P("ep", "tp", None),
            P("ep", None, "tp"),
            P("tp", None),
            P("tp", None),
            P(None, "tp"),
            P("tp"),
        ),
        out_specs=P(("grp", "ep"), "tp"),
        check_vma=False,
    )
```
